256 devices in a mesh: grp: 2 (over y), fs: 16 (over z), tp: 8 (over x, core).
Axes of the slice: x: 4, y: 2, z: 16, core: 2. Of those that a mesh axis runs over, the one named last changes fastest.
The devices are a block of a 4x16x16 slice.
Arguments:
- tokens: bfloat16 [32768, 2048], P(('grp', 'fs'), 'tp'), parts along dimension 0, may hold values from -6 to 6
- mixer_gain: float32 [2048], replicated, may hold values from 0.1 to 1.9
- branch_weight: float32 [2048, 1024], P('fs', 'tp'), may hold values from -0.125 to 0.125
- gelu_weight: float32 [2048, 1024], P('fs', 'tp'), may hold values from -0.125 to 0.125
- branch_scale: float32 [16, 64], P('fs', 'tp'), may hold values from 0.5 to 2
- gelu_scale: float32 [16, 64], P('fs', 'tp'), may hold values from 0.5 to 2
- branch_taps: float32 [4, 1024], P(None, 'tp'), may hold values from -3 to 3
- recur_gate: bfloat16 [16, 64, 64], P('tp'), may hold values from -0.75 to 0.75
- input_gate: bfloat16 [16, 64, 64], P('tp'), may hold values from -0.75 to 0.75
- decay_param: float32 [1024], P('tp'), may hold values from 4 to 7
- out_weight: float32 [1024, 2048], P('tp', 'fs'), may hold values from -0.5 to 0.5
- out_scale: float32 [16, 128], P('fs'), may hold values from 0.5 to 2
- ffn_gain: float32 [2048], replicated, may hold values from 0.1 to 1.9
- upgate_weight: float32 [2048, 5632], P('fs', 'tp'), may hold values from -0.125 to 0.125
- upval_weight: float32 [2048, 5632], P('fs', 'tp'), may hold values from -0.125 to 0.125
- upgate_scale: float32 [16, 352], P('fs', 'tp'), may hold values from 0.5 to 2
- upval_scale: float32 [16, 352], P('fs', 'tp'), may hold values from 0.5 to 2
- upgate_taps: float32 [3, 5632], P(None, 'tp'), may hold values from -3 to 3
- upval_taps: float32 [3, 5632], P(None, 'tp'), may hold values from -3 to 3
- down_weight: float32 [5632, 2048], P('tp', 'fs'), may hold values from -0.15625 to 0.15625
- down_scale: float32 [16, 128], P('fs'), may hold values from 0.5 to 2
Outputs:
- layer_out: bfloat16 [32768, 2048], P(('grp', 'fs'), 'tp'), parts along dimension 0
The draws below stay inside these ranges and needn't reach their ends.
There are 2 independent parts, one for each index of `grp`. The reference program is written for one: setup_inputs(seed, part) draws one part's arguments, and reference() takes and returns one part's arrays. A program takes and returns all parts, laid end to end along the dimension named above; an argument that names none is the same for every part. Nothing has to cross between parts.
All inputs are finite; a program needn't handle non-finite values.
Results may differ from the reference program's by a relative error of at most 0.024.
Values may be sent and summed in bfloat16 or wider, within the bound.
No kernel may reach another device: no remote copies, remote signals or barrier semaphores. Data moves between devices by JAX's collectives and lax.ppermute only.
A program may use at most 128 MiB of HBM per device.

```python
import math
import jax
import jax.numpy as jnp
from jax import lax

D = 2048
LRU = 1024
LRU_BLOCK = 64
NB = 16
CONV_LRU = 4
FF = 5632
CONV_FF = 3
SEQ_LEN = 512
TOKENS = 16384
N_FS = 16
N_TP = 8


def draw_decay_param(key, part):
    pick_key, slow_key, fast_key = jax.random.split(jax.random.fold_in(key, 11), 3)
    share = 0.5
    chooser = jax.random.uniform(pick_key, (LRU,), jnp.float32)
    slow_vals = jax.random.uniform(slow_key, (LRU,), jnp.float32, 6.0, 7.0)
    fast_vals = jax.random.uniform(fast_key, (LRU,), jnp.float32, 4.0, 5.0)
    return jnp.where(chooser < share, slow_vals, fast_vals).astype(jnp.float32)


def shard_levels(own_key, shape, pieces, smallest, high):
    level, own = 1.0, jax.random.fold_in(own_key, 6)
    for position, blocks in pieces:
        steps = jnp.exp(jax.random.uniform(jax.random.fold_in(own, position), (blocks,), jnp.float32, smallest / len(pieces), high / len(pieces)))
        level = level * jnp.repeat(steps, shape[position] // blocks).reshape([-1 if axis == position else 1 for axis in range(len(shape))])
    return level


def centred(stream_key, dims, scale, limit, shards=(), kind=jnp.bfloat16):
    entries = jax.random.normal(stream_key, dims, jnp.float32) * scale
    if len(shards) > 0:
        entries = shard_levels(stream_key, dims, shards, -0.22, 0.18) * entries
    return jnp.clip(entries, min=-limit, max=limit).astype(kind)


def setup_inputs(seed: int = 0, part: int = 0) -> dict:
    streams_of = jax.random.split(jax.random.key(seed), 22)
    own_keys = jax.random.split(jax.random.fold_in(streams_of[21], part), 22)
    return {
        "tokens": centred(own_keys[0], (TOKENS, D), 1.0, 6.0, ((0, 16), (1, 8))),
        "mixer_gain": jnp.clip(1.0 + 0.18 * jax.random.normal(streams_of[1], (D,), jnp.float32), 0.1, 1.9),
        "branch_weight": centred(streams_of[2], (D, LRU), D ** -0.5, 0.125, ((0, 16), (1, 8)), jnp.float32),
        "gelu_weight": centred(streams_of[3], (D, LRU), D ** -0.5, 0.125, ((0, 16), (1, 8)), jnp.float32),
        "branch_scale": jnp.clip(jnp.exp(math.log(2.0) - 1.3862944 * jax.random.uniform(streams_of[4], (N_FS, LRU // N_FS), jnp.float32) ** shard_levels(streams_of[4], (N_FS, LRU // N_FS), ((0, 16), (1, 8)), -0.2, 0.2)), 0.5, 2.0),
        "gelu_scale": jnp.clip(jnp.exp(math.log(2.0) - 1.3862944 * jax.random.uniform(streams_of[5], (N_FS, LRU // N_FS), jnp.float32) ** shard_levels(streams_of[5], (N_FS, LRU // N_FS), ((0, 16), (1, 8)), -0.2, 0.2)), 0.5, 2.0),
        "branch_taps": centred(streams_of[6], (CONV_LRU, LRU), 0.5, 3.0, ((1, 8),), jnp.float32),
        "recur_gate": centred(streams_of[7], (NB, LRU_BLOCK, LRU_BLOCK), LRU_BLOCK ** -0.5, 0.75, ((0, 8),)),
        "input_gate": centred(streams_of[8], (NB, LRU_BLOCK, LRU_BLOCK), LRU_BLOCK ** -0.5, 0.75, ((0, 8),)),
        "decay_param": draw_decay_param(jax.random.fold_in(streams_of[21], 71), part),
        "out_weight": centred(streams_of[10], (LRU, D), (LRU // 8) ** -0.5, 0.5, ((0, 8), (1, 16)), jnp.float32),
        "out_scale": jnp.clip(jnp.exp(math.log(2.0) - 1.3862944 * jax.random.uniform(streams_of[11], (N_FS, D // N_FS), jnp.float32) ** shard_levels(streams_of[11], (N_FS, D // N_FS), ((0, 16),), -0.2, 0.2)), 0.5, 2.0),
        "ffn_gain": jnp.clip(1.0 + 0.18 * jax.random.normal(streams_of[12], (D,), jnp.float32), 0.1, 1.9),
        "upgate_weight": centred(streams_of[13], (D, FF), D ** -0.5, 0.125, ((0, 16), (1, 8)), jnp.float32),
        "upval_weight": centred(streams_of[14], (D, FF), D ** -0.5, 0.125, ((0, 16), (1, 8)), jnp.float32),
        "upgate_scale": jnp.clip(jnp.exp(math.log(2.0) - 1.3862944 * jax.random.uniform(streams_of[15], (N_FS, FF // N_FS), jnp.float32) ** shard_levels(streams_of[15], (N_FS, FF // N_FS), ((0, 16), (1, 8)), -0.2, 0.2)), 0.5, 2.0),
        "upval_scale": jnp.clip(jnp.exp(math.log(2.0) - 1.3862944 * jax.random.uniform(streams_of[16], (N_FS, FF // N_FS), jnp.float32) ** shard_levels(streams_of[16], (N_FS, FF // N_FS), ((0, 16), (1, 8)), -0.2, 0.2)), 0.5, 2.0),
        "upgate_taps": centred(streams_of[17], (CONV_FF, FF), 0.577, 3.0, ((1, 8),), jnp.float32),
        "upval_taps": centred(streams_of[18], (CONV_FF, FF), 0.577, 3.0, ((1, 8),), jnp.float32),
        "down_weight": centred(streams_of[19], (FF, D), (FF // 4) ** -0.5, 0.15625, ((0, 8), (1, 16)), jnp.float32),
        "down_scale": jnp.clip(jnp.exp(math.log(2.0) - 1.3862944 * jax.random.uniform(streams_of[20], (N_FS, D // N_FS), jnp.float32) ** shard_levels(streams_of[20], (N_FS, D // N_FS), ((0, 16),), -0.2, 0.2)), 0.5, 2.0),
    }


def rms_rows(values_in, norm_gain):
    values = values_in.astype(jnp.float32)
    inverse = lax.rsqrt(lax.optimization_barrier(jnp.mean(values * values, axis=-1, keepdims=True)) + 1e-06)
    return (values * inverse * norm_gain.astype(jnp.float32)).astype(jnp.bfloat16)

def col_scale(scale_table):
    return scale_table.T.reshape(-1)

def causal_mix(values, filter_taps, seq_len):
    columns = values.shape[-1]
    grouped = values.reshape(-1, seq_len, columns)
    tap_count = filter_taps.shape[0]
    padded = jnp.pad(grouped, ((0, 0), (tap_count - 1, 0), (0, 0)))
    totals = padded[:, 0:seq_len] * filter_taps[0]
    for k in range(1, tap_count):
        totals = totals + padded[:, k:k + seq_len] * filter_taps[k]
    return totals.reshape(-1, columns)

def combine_pairs(earlier, later):
    return (earlier[0] * later[0], later[0] * earlier[1] + later[1])

def run_scan(factors, inputs, seq_len):
    columns = factors.shape[-1]
    pair = (factors.reshape(-1, seq_len, columns), inputs.reshape(-1, seq_len, columns))
    _, states = lax.associative_scan(combine_pairs, pair, axis=1)
    return states.reshape(-1, columns)

def block_sum(left, weight, scales, parts):
    block_rows = left.shape[1] // parts
    totals = jnp.zeros((left.shape[0], weight.shape[1]), jnp.float32)
    for index in range(parts):
        partial_value = jnp.dot(left[:, index * block_rows:(index + 1) * block_rows], weight[index * block_rows:(index + 1) * block_rows], preferred_element_type=jnp.float32) * scales
        totals = totals + lax.optimization_barrier(partial_value.astype(jnp.bfloat16)).astype(jnp.float32)
    return totals

def reference(tokens, mixer_gain, branch_weight, gelu_weight, branch_scale, gelu_scale, branch_taps, recur_gate, input_gate, decay_param, out_weight, out_scale, ffn_gain, upgate_weight, upval_weight, upgate_scale, upval_scale, upgate_taps, upval_taps, down_weight, down_scale):
    normed = rms_rows(tokens, mixer_gain)
    branch = jnp.dot(normed, branch_weight.astype(jnp.bfloat16), preferred_element_type=jnp.float32) * col_scale(branch_scale)
    gelu_in = jnp.dot(normed, gelu_weight.astype(jnp.bfloat16), preferred_element_type=jnp.float32) * col_scale(gelu_scale)
    convolved = causal_mix(branch, branch_taps, SEQ_LEN).astype(jnp.bfloat16)
    blocks = convolved.astype(jnp.float32).reshape(-1, NB, LRU_BLOCK)
    recur = jax.nn.sigmoid(jnp.einsum('rnc,ncd->rnd', blocks, recur_gate.astype(jnp.float32)).reshape(-1, LRU))
    input_rate = jax.nn.sigmoid(jnp.einsum('rnc,ncd->rnd', blocks, input_gate.astype(jnp.float32)).reshape(-1, LRU))
    log_decay = -8.0 * recur * jax.nn.softplus(-decay_param)
    decay_rate = jnp.exp(log_decay)
    driven = jnp.sqrt(-jnp.expm1(2.0 * log_decay)) * input_rate * convolved.astype(jnp.float32)
    states = run_scan(decay_rate, driven, SEQ_LEN)
    gated_state = (states * jax.nn.gelu(gelu_in)).astype(jnp.bfloat16)
    mixer_sum = block_sum(gated_state, out_weight.astype(jnp.bfloat16), col_scale(out_scale), N_TP)
    hidden_state = (tokens.astype(jnp.float32) + mixer_sum).astype(jnp.bfloat16)
    normed_ffn = rms_rows(hidden_state, ffn_gain)
    up_gate = jnp.dot(normed_ffn, upgate_weight.astype(jnp.bfloat16), preferred_element_type=jnp.float32) * col_scale(upgate_scale)
    up_val = jnp.dot(normed_ffn, upval_weight.astype(jnp.bfloat16), preferred_element_type=jnp.float32) * col_scale(upval_scale)
    conv_gate = causal_mix(up_gate, upgate_taps, SEQ_LEN)
    conv_val = causal_mix(up_val, upval_taps, SEQ_LEN)
    ffn_hidden = (jax.nn.silu(conv_gate) * conv_val).astype(jnp.bfloat16)
    ffn_sum = block_sum(ffn_hidden, down_weight.astype(jnp.bfloat16), col_scale(down_scale), N_TP)
    return (hidden_state.astype(jnp.float32) + ffn_sum).astype(jnp.bfloat16)
```

```python
import functools
import jax
import jax.numpy as jnp
from jax import lax
from jax.experimental import pallas as pl
from jax.experimental.pallas import tpu as pltpu
from jax.sharding import PartitionSpec as P

SEQ_LEN = 512
EPS = 1e-06
BF = jnp.bfloat16
F32 = jnp.float32
LANES = 128
CORES = 2
SLOTS = ((0, 0), (1, 0), (-1, 0), (2, 0), (0, 1), (1, 1), (-1, 1), (2, 1))
HALF_SLOTS = 4
SCALE_ROWS = 16
PIECES = 3


def from_chip(value, step):
    size = lax.axis_size("tp")
    chips = size // CORES
    pairs = [(i, ((i // CORES - step) % chips) * CORES + i % CORES) for i in range(size)]
    return lax.ppermute(value, "tp", pairs)


def from_partner(value):
    size = lax.axis_size("tp")
    return lax.ppermute(value, "tp", [(i, i ^ 1) for i in range(size)])


def gather_tp(value):
    half = value.shape[0] // 2
    right = from_chip(value, 1)
    left = from_chip(value, -1)
    far = jnp.concatenate([from_chip(right[:half], 1), from_chip(left[half:], -1)], axis=0)
    same = [value, right, left, far]
    return same + [from_partner(piece) for piece in same]


def ring_fs(shard, cut):
    size = lax.axis_size("fs")
    up = [(i, (i + 1) % size) for i in range(size)]
    down = [(i, (i - 1) % size) for i in range(size)]
    below, above = [shard], [shard]
    for _ in range(size // 2 - 1):
        below.append(lax.ppermute(below[-1], "fs", up))
        above.append(lax.ppermute(above[-1], "fs", down))
    far = jnp.concatenate(
        [lax.ppermute(below[-1][:cut], "fs", up), lax.ppermute(above[-1][cut:], "fs", down)], axis=0
    )
    return above + [far] + below[:0:-1]


def slot_device(tp, slot):
    step, other = slot
    core = lax.rem(tp, CORES)
    chip = lax.rem(lax.div(tp, CORES) + step + HALF_SLOTS, HALF_SLOTS)
    return chip * CORES + (1 - core if other else core)


def shift_rows(values, by, fill):
    rows = lax.broadcasted_iota(jnp.int32, values.shape, 0)
    return jnp.where(rows >= by, pltpu.roll(values, by, 0), fill)


def causal_mix(values, taps):
    count = taps.shape[0]
    total = values * taps[count - 1 : count]
    for by in range(1, count):
        total = total + shift_rows(values, by, 0.0) * taps[count - 1 - by : count - by]
    return total


def spread_scale(table, group, first, fs, second=None):
    shape = (LANES, LANES)
    lane = lax.broadcasted_iota(jnp.int32, shape, 1)
    row = lax.broadcasted_iota(jnp.int32, shape, 0)
    wanted = first + lax.shift_right_logical(lane, 4)
    if second is not None:
        wanted = jnp.where(lane < LANES // 2, wanted, second + lax.shift_right_logical(lane, 4) - 4)
    pick = jnp.where(row == wanted, 1.0, 0.0).astype(BF)
    hits = jnp.dot(table, pick, preferred_element_type=F32)
    row = lax.broadcasted_iota(jnp.int32, hits.shape, 0)
    lane = lax.broadcasted_iota(jnp.int32, hits.shape, 1)
    owner = lax.bitwise_and(lax.shift_right_logical(row, 4) + fs, 15)
    local = lax.bitwise_and(row, SCALE_ROWS - 1)
    keep = (
        (owner == lax.bitwise_and(lane, 15))
        & (local >= group * PIECES)
        & (local < group * PIECES + PIECES)
    )
    return jnp.sum(jnp.where(keep, hits, 0.0), axis=0, keepdims=True)


def minus_expm1(x):
    series = x * (
        1.0
        + x
        * (0.5 + x * (1.0 / 6 + x * (1.0 / 24 + x * (1.0 / 120 + x * (1.0 / 720 + x / 5040)))))
    )
    return jnp.where(x > -0.5, -series, 1.0 - jnp.exp(x))


def scan_rows(factors, inputs):
    by = 1
    while by < factors.shape[0]:
        if by < 8:
            before_f, before_i = shift_rows(factors, by, 1.0), shift_rows(inputs, by, 0.0)
        else:
            top = (by, factors.shape[1])
            before_f = jnp.concatenate([jnp.ones(top, F32), factors[:-by]], axis=0)
            before_i = jnp.concatenate([jnp.zeros(top, F32), inputs[:-by]], axis=0)
        inputs = factors * before_i + inputs
        factors = factors * before_f
        by *= 2
    return inputs


def pack_mixer_kernel(branch_ref, gelu_ref, out_ref, scale_ref, packed_ref):
    rows = branch_ref.shape[0]
    packed_ref[0:rows] = branch_ref[...].astype(BF)
    packed_ref[rows : 2 * rows] = gelu_ref[...].astype(BF)
    scales = scale_ref[...]
    high = scales.astype(BF)
    rest = scales - high.astype(F32)
    middle = rest.astype(BF)
    low = (rest - middle.astype(F32)).astype(BF)
    parts = []
    for group in range(scales.shape[0]):
        for piece in (high, middle, low):
            parts.append(piece[group : group + 1].astype(F32))
    parts.append(jnp.zeros((SCALE_ROWS - len(parts), LANES), F32))
    packed_ref[2 * rows : 2 * rows + SCALE_ROWS] = jnp.concatenate(parts, axis=0).astype(BF)
    packed_ref[2 * rows + SCALE_ROWS :] = out_ref[...].astype(BF)


def pack_ffn_kernel(gate_ref, value_ref, down_ref, packed_ref):
    rows, width = gate_ref.shape
    whole = width // LANES
    for j in range(whole):
        cols = slice(j * LANES, (j + 1) * LANES)
        packed_ref[2 * j * rows : (2 * j + 1) * rows] = gate_ref[:, cols].astype(BF)
        packed_ref[(2 * j + 1) * rows : (2 * j + 2) * rows] = value_ref[:, cols].astype(BF)
    mixed = jnp.concatenate([gate_ref[:, whole * LANES :], value_ref[:, whole * LANES :]], axis=1)
    packed_ref[2 * whole * rows : (2 * whole + 1) * rows] = mixed.astype(BF)
    packed_ref[(2 * whole + 1) * rows :] = down_ref[...].astype(BF)


def mixer_kernel(pos_ref, *refs):
    tokens = refs[:8]
    w_ref, gain_ref, taps_ref, gates_ref, rate_ref, out_ref, x_ref, full_ref, scale_ref = refs[8:]
    tp, fs = pos_ref[0], pos_ref[1]
    size = w_ref.shape[0]
    width = tokens[0].shape[1]
    per_slot = width // LANES

    @pl.when(pl.program_id(0) == 0)
    def _():
        for slot, place in enumerate(SLOTS):
            device = slot_device(tp, place)
            for part in range(per_slot):
                at = lax.rem(device * per_slot + part - fs + size, size)
                base = slot * width + part * LANES
                full_ref[base : base + LANES, :LANES] = w_ref[at, :LANES]
                full_ref[base : base + LANES, LANES:] = w_ref[at, LANES : 2 * LANES]
        table = w_ref[:, 2 * LANES :].reshape(size * SCALE_ROWS, LANES)
        scale_ref[:, :LANES] = spread_scale(table, 0, 0, fs)
        scale_ref[:, LANES:] = spread_scale(table, 0, 8, fs)

    squares = None
    for slot in range(len(SLOTS)):
        values = tokens[slot][...].astype(F32)
        square = jnp.sum(values * values, axis=-1, keepdims=True)
        squares = square if squares is None else squares + square
    inverse = lax.rsqrt(squares * (1.0 / x_ref.shape[1]) + EPS)
    for slot, place in enumerate(SLOTS):
        values = tokens[slot][...].astype(F32)
        gain = gain_ref[slot_device(tp, place)]
        x_ref[:, slot * width : (slot + 1) * width] = (values * inverse * gain).astype(BF)
    both = jnp.dot(x_ref[...], full_ref[...], preferred_element_type=F32)
    taps = taps_ref[...] * scale_ref[:, :LANES]
    convolved = causal_mix(both[:, :LANES], taps).astype(BF)
    rates = jax.nn.sigmoid(jnp.dot(convolved, gates_ref[...], preferred_element_type=F32))
    log_decay = rates[:, :LANES] * rate_ref[...]
    driven = jnp.sqrt(minus_expm1(2.0 * log_decay)) * rates[:, LANES:] * convolved.astype(F32)
    states = scan_rows(jnp.exp(log_decay), driven)
    gelu_in = both[:, LANES:] * scale_ref[:, LANES:]
    out_ref[...] = (states * jax.nn.gelu(gelu_in)).astype(BF)


def out_kernel(pos_ref, *refs):
    tokens, gated, weights = refs[:8], refs[8:16], refs[16:24]
    (s_ref, gain_ref, taps_ref, normed_ref, own_ref, mixed_ref, down_ref, full_ref, scale_ref,
     hidden_ref) = refs[24:]
    tp, fs = pos_ref[0], pos_ref[1]
    size = s_ref.shape[0]
    width = tokens[0].shape[1]
    per_slot = width // LANES

    @pl.when(pl.program_id(0) == 0)
    def _():
        table = s_ref[...].reshape(size * SCALE_ROWS, LANES)
        for slot, place in enumerate(SLOTS):
            device = slot_device(tp, place)
            for part in range(per_slot):
                block = device * per_slot + part
                at = lax.rem(block - fs + size, size)
                cols = slice(slot * width + part * LANES, slot * width + (part + 1) * LANES)
                for row_slot in range(len(SLOTS)):
                    full_ref[row_slot * LANES : (row_slot + 1) * LANES, cols] = weights[row_slot][at]
                scale_ref[:, cols] = spread_scale(table, 1, block * 8, fs)
                if slot == 0:
                    down_ref[:, cols] = spread_scale(table, 2, block * 8, fs)
        gate_at, value_at = 16, 60
        pairs = (mixed_ref.shape[1] // LANES) // 2
        for j in range(pairs):
            cols = slice(2 * j * LANES, (2 * j + 1) * LANES)
            mixed_ref[:, cols] = taps_ref[:, cols] * spread_scale(table, 0, gate_at + 8 * j, fs)
            cols = slice((2 * j + 1) * LANES, (2 * j + 2) * LANES)
            mixed_ref[:, cols] = taps_ref[:, cols] * spread_scale(table, 0, value_at + 8 * j, fs)
        cols = slice(2 * pairs * LANES, (2 * pairs + 1) * LANES)
        mixed_ref[:, cols] = taps_ref[:, cols] * spread_scale(
            table, 0, gate_at + 8 * pairs, fs, value_at + 8 * pairs
        )

    states = jnp.concatenate([ref[...] for ref in gated], axis=1)
    squares = None
    for slot in range(len(SLOTS)):
        cols = slice(slot * width, (slot + 1) * width)
        mixed = jnp.dot(states, full_ref[:, cols], preferred_element_type=F32)
        mixed = mixed * scale_ref[:, cols]
        hidden = (tokens[slot][...].astype(F32) + mixed).astype(BF)
        hidden_ref[:, cols] = hidden
        if slot == 0:
            own_ref[...] = hidden
        values = hidden.astype(F32)
        square = jnp.sum(values * values, axis=-1, keepdims=True)
        squares = square if squares is None else squares + square
    inverse = lax.rsqrt(squares * (1.0 / hidden_ref.shape[1]) + EPS)
    for slot, place in enumerate(SLOTS):
        device = slot_device(tp, place)
        values = hidden_ref[:, slot * width : (slot + 1) * width].astype(F32)
        normed_ref[device] = (values * inverse * gain_ref[device]).astype(BF)


def ffn_kernel(pos_ref, x_ref, w_ref, taps_ref, send_ref, keep_ref, hidden_ref):
    tp = pos_ref[0]
    count, rows, width = x_ref.shape
    per_slot = width // LANES
    up_rows = taps_ref.shape[1]
    pairs = (up_rows // LANES) // 2
    depth = count * width

    def columns(j):
        return w_ref[:, j * LANES : (j + 1) * LANES].reshape(depth, LANES)

    x = jnp.concatenate([x_ref[k] for k in range(count)], axis=1)
    for j in range(pairs):
        weight = jnp.concatenate([columns(2 * j), columns(2 * j + 1)], axis=1)
        both = jnp.dot(x, weight, preferred_element_type=F32)
        both = causal_mix(both, taps_ref[:, 2 * j * LANES : (2 * j + 2) * LANES])
        gate = both[:, :LANES]
        hidden_ref[:, j * LANES : (j + 1) * LANES] = (
            gate * jax.nn.sigmoid(gate) * both[:, LANES:]
        ).astype(BF)
    both = jnp.dot(x, columns(2 * pairs), preferred_element_type=F32)
    both = causal_mix(both, taps_ref[:, 2 * pairs * LANES :])
    product = both * jax.nn.sigmoid(both) * pltpu.roll(both, LANES // 2, 1)
    hidden_ref[:, pairs * LANES :] = product[:, : LANES // 2].astype(BF)
    hidden = hidden_ref[...]
    for slot, place in enumerate(SLOTS):
        device = slot_device(tp, place)
        weight = jnp.concatenate(
            [w_ref[device * per_slot + part, up_rows:] for part in range(per_slot)], axis=1
        )
        term = jnp.dot(hidden, weight, preferred_element_type=F32).astype(BF)
        target = keep_ref if slot < HALF_SLOTS else send_ref
        target[slot % HALF_SLOTS] = term


def whole(array):
    rank = array.ndim
    return pl.BlockSpec(array.shape, lambda i, pos: (0,) * rank, pipeline_mode=pl.Buffered(1))


def row_block(rows, width):
    return pl.BlockSpec((rows, width), lambda i, pos: (i, 0))


def slab(count, rows, width):
    return pl.BlockSpec((count, rows, width), lambda i, pos: (0, i, 0))


def fixed(shape):
    rank = len(shape)
    return pl.BlockSpec(shape, lambda i, pos: (0,) * rank)


def call(kernel, position, steps, operands, in_specs, outs, out_specs, scratch, flops, name):
    size = sum(a.size * a.dtype.itemsize for a in operands)
    return pl.pallas_call(
        kernel,
        grid_spec=pltpu.PrefetchScalarGridSpec(
            num_scalar_prefetch=1,
            grid=(steps,),
            in_specs=in_specs,
            out_specs=out_specs,
            scratch_shapes=scratch,
        ),
        out_shape=outs,
        compiler_params=pltpu.CompilerParams(dimension_semantics=("arbitrary",)),
        cost_estimate=pl.CostEstimate(flops=flops, transcendentals=0, bytes_accessed=size),
        name=name,
    )(position, *operands)


def block_diagonal(blocks):
    count, size, _ = blocks.shape
    rows = []
    for i in range(count):
        rows.append(jnp.pad(blocks[i], ((0, 0), (i * size, (count - 1 - i) * size))))
    return jnp.concatenate(rows, axis=0)


def per_device(
    tokens,
    mixer_gain,
    branch_weight,
    gelu_weight,
    branch_scale,
    gelu_scale,
    branch_taps,
    recur_gate,
    input_gate,
    decay_param,
    out_weight,
    out_scale,
    ffn_gain,
    upgate_weight,
    upval_weight,
    upgate_scale,
    upval_scale,
    upgate_taps,
    upval_taps,
    down_weight,
    down_scale,
):
    fs_size, tp_size = lax.axis_size("fs"), lax.axis_size("tp")
    rows, width = tokens.shape
    depth = width * tp_size
    steps = rows // SEQ_LEN
    position = jnp.stack([lax.axis_index("tp"), lax.axis_index("fs")]).astype(jnp.int32)

    hidden_width = upgate_weight.shape[1]
    up_rows = 2 * hidden_width * upgate_weight.shape[0] // LANES
    packed_ffn = pl.pallas_call(
        pack_ffn_kernel,
        out_shape=jax.ShapeDtypeStruct((up_rows + hidden_width, LANES), BF),
        name="pack_ffn",
    )(upgate_weight, upval_weight, down_weight)
    ffn_weights = lax.all_gather(packed_ffn, "fs", axis=0, tiled=True)
    ffn_weights = ffn_weights.reshape(fs_size, up_rows + hidden_width, LANES)

    small = jnp.concatenate([branch_scale, gelu_scale, upgate_scale, upval_scale], axis=1)
    small = jnp.pad(small, ((0, 0), (0, LANES - small.shape[1])))
    scales = jnp.concatenate([small, out_scale, down_scale], axis=0)
    front = 2 * LANES + SCALE_ROWS
    packed_mixer = pl.pallas_call(
        pack_mixer_kernel,
        out_shape=jax.ShapeDtypeStruct((front + LANES, LANES), BF),
        name="pack_mixer",
    )(branch_weight, gelu_weight, out_weight, scales)

    token_slots = gather_tp(tokens)
    pieces = ring_fs(packed_mixer, 208)
    mixer_weights = jnp.stack([piece[:front] for piece in pieces])
    scale_rows = mixer_weights[:, 2 * LANES :]
    out_rows = jnp.concatenate([piece[front:] for piece in pieces], axis=0)
    out_slots = [v.reshape(fs_size, LANES, LANES) for v in gather_tp(out_rows)]

    gates = jnp.concatenate([block_diagonal(recur_gate), block_diagonal(input_gate)], axis=1)
    rate = (-8.0 * jax.nn.softplus(-decay_param))[None]
    mixer_gains = mixer_gain.reshape(tp_size, 1, width)
    ffn_gains = ffn_gain.reshape(tp_size, 1, width)
    token_specs = [row_block(SEQ_LEN, width)] * len(SLOTS)

    tail = (mixer_weights, mixer_gains, branch_taps, gates, rate)
    gated = call(
        mixer_kernel,
        position,
        steps,
        (*token_slots, *tail),
        token_specs + [whole(a) for a in tail],
        jax.ShapeDtypeStruct((rows, LANES), BF),
        row_block(SEQ_LEN, LANES),
        [
            pltpu.VMEM((SEQ_LEN, depth), BF),
            pltpu.VMEM((depth, 2 * LANES), BF),
            pltpu.VMEM((1, 2 * LANES), F32),
        ],
        2 * rows * depth * 2 * LANES,
        "mixer",
    )
    gated_slots = gather_tp(gated)

    edge = hidden_width // LANES * LANES
    tap_parts = []
    for j in range(hidden_width // LANES):
        tap_parts += [upgate_taps[:, j * LANES : (j + 1) * LANES]]
        tap_parts += [upval_taps[:, j * LANES : (j + 1) * LANES]]
    tap_parts += [upgate_taps[:, edge:], upval_taps[:, edge:]]
    ffn_taps = jnp.concatenate(tap_parts, axis=1)

    block = SEQ_LEN // 2
    tail = (scale_rows, ffn_gains, ffn_taps)
    normed, own_hidden, scaled_taps, down_cols = call(
        out_kernel,
        position,
        rows // block,
        (*token_slots, *gated_slots, *out_slots, *tail),
        [row_block(block, width)] * len(SLOTS)
        + [row_block(block, LANES)] * len(SLOTS)
        + [whole(a) for a in (*out_slots, *tail)],
        (
            jax.ShapeDtypeStruct((tp_size, rows, width), BF),
            jax.ShapeDtypeStruct((rows, width), BF),
            jax.ShapeDtypeStruct(ffn_taps.shape, F32),
            jax.ShapeDtypeStruct((1, width), F32),
        ),
        (
            slab(tp_size, block, width),
            row_block(block, width),
            fixed(ffn_taps.shape),
            fixed((1, width)),
        ),
        [
            pltpu.VMEM((tp_size * LANES, depth), BF),
            pltpu.VMEM((1, depth), F32),
            pltpu.VMEM((block, depth), BF),
        ],
        2 * rows * tp_size * LANES * depth,
        "out_proj",
    )

    term = jax.ShapeDtypeStruct((HALF_SLOTS, rows, width), BF)
    send, keep = call(
        ffn_kernel,
        position,
        steps,
        (normed, ffn_weights, scaled_taps),
        [slab(tp_size, SEQ_LEN, width), whole(ffn_weights), whole(scaled_taps)],
        (term, term),
        (slab(HALF_SLOTS, SEQ_LEN, width), slab(HALF_SLOTS, SEQ_LEN, width)),
        [pltpu.VMEM((SEQ_LEN, hidden_width), BF)],
        6 * rows * depth * hidden_width,
        "ffn",
    )
    received = from_partner(send)
    sums = [
        (keep[k].astype(F32) + received[k].astype(F32)).astype(BF) for k in range(HALF_SLOTS)
    ]
    total = sums[0].astype(F32)
    for k in range(1, HALF_SLOTS):
        total = total + from_chip(sums[k], -SLOTS[k][0]).astype(F32)
    return (own_hidden.astype(F32) + total * down_cols).astype(BF)


def solution(mesh):
    in_specs = (
        P(("grp", "fs"), "tp"),
        P(),
        P("fs", "tp"),
        P("fs", "tp"),
        P("fs", "tp"),
        P("fs", "tp"),
        P(None, "tp"),
        P("tp", None, None),
        P("tp", None, None),
        P("tp"),
        P("tp", "fs"),
        P("fs", None),
        P(),
        P("fs", "tp"),
        P("fs", "tp"),
        P("fs", "tp"),
        P("fs", "tp"),
        P(None, "tp"),
        P(None, "tp"),
        P("tp", "fs"),
        P("fs", None),
    )
    out_specs = P(("grp", "fs"), "tp")
    return jax.shard_map(
        per_device, mesh=mesh, in_specs=in_specs, out_specs=out_specs, check_vma=False
    )
```

```python
import jax
import jax.numpy as jnp
from jax import lax
from jax.experimental import pallas as pl
from jax.experimental.pallas import tpu as pltpu
from jax.sharding import PartitionSpec as P

SEQ_LEN = 512
EPS = 1e-06
BF = jnp.bfloat16
F32 = jnp.float32
LANES = 128
CORES = 2
SLOTS = ((0, 0), (1, 0), (2, 0), (3, 0), (0, 1), (1, 1), (2, 1), (3, 1))
HALF_SLOTS = 4
SCALE_ROWS = 16
PIECES = 3


def from_chip(value, step):
    size = lax.axis_size("tp")
    chips = size // CORES
    pairs = [(i, ((i // CORES - step) % chips) * CORES + i % CORES) for i in range(size)]
    return lax.ppermute(value, "tp", pairs)


def from_partner(value):
    size = lax.axis_size("tp")
    return lax.ppermute(value, "tp", [(i, i ^ 1) for i in range(size)])


def near_chips(value):
    return from_chip(value, 1), from_chip(value, -1)


def far_chip(right, left):
    half = right.shape[0] // 2
    return from_chip(right[:half], 1), from_chip(left[half:], -1)


def complete_tp(value, right, left, far):
    same = jnp.stack([value, right, jnp.concatenate(far, axis=0), left])
    return same, from_partner(same)


def gather_directly(value):
    size = lax.axis_size("tp")
    chips = size // CORES
    slots = [value]
    for step, other in SLOTS[1:]:
        pairs = [
            (i, ((i // CORES - step) % chips) * CORES + (i % CORES) ^ other) for i in range(size)
        ]
        slots.append(lax.ppermute(value, "tp", pairs))
    return slots


def ring_fs(shard, cut):
    size = lax.axis_size("fs")
    up = [(i, (i + 1) % size) for i in range(size)]
    down = [(i, (i - 1) % size) for i in range(size)]
    stack = jnp.zeros((size, *shard.shape), shard.dtype)
    stack = lax.dynamic_update_slice_in_dim(stack, shard[None], 0, 0)

    def held(stack, below, above, k):
        stack = lax.dynamic_update_slice_in_dim(stack, above[None], k, 0)
        return lax.dynamic_update_slice_in_dim(stack, below[None], size - k, 0)

    def step(k, state):
        stack, below, above = state
        next_below = lax.ppermute(below, "fs", up)
        next_above = lax.ppermute(above, "fs", down)
        return held(stack, below, above, k), next_below, next_above

    first = (lax.ppermute(shard, "fs", up), lax.ppermute(shard, "fs", down))
    stack, below, above = lax.fori_loop(1, size // 2 - 1, step, (stack, *first))
    far_top = lax.ppermute(below[:cut], "fs", up)
    far_bottom = lax.ppermute(above[cut:], "fs", down)
    stack = held(stack, below, above, size // 2 - 1)
    far = jnp.concatenate([far_top, far_bottom], axis=0)
    return lax.dynamic_update_slice_in_dim(stack, far[None], size // 2, 0)


def slot_device(tp, slot):
    step, other = slot
    core = lax.rem(tp, CORES)
    chip = lax.rem(lax.div(tp, CORES) + step + HALF_SLOTS, HALF_SLOTS)
    return chip * CORES + (1 - core if other else core)


def shift_rows(values, by, fill):
    rows = lax.broadcasted_iota(jnp.int32, values.shape, 0)
    return jnp.where(rows >= by, pltpu.roll(values, by, 0), fill)


def causal_mix(values, taps):
    count = taps.shape[0]
    total = values * taps[count - 1 : count]
    for by in range(1, count):
        total = total + shift_rows(values, by, 0.0) * taps[count - 1 - by : count - by]
    return total


def spread_scale(table, group, first, fs, second=None):
    shape = (LANES, LANES)
    lane = lax.broadcasted_iota(jnp.int32, shape, 1)
    row = lax.broadcasted_iota(jnp.int32, shape, 0)
    wanted = first + lax.shift_right_logical(lane, 4)
    if second is not None:
        wanted = jnp.where(lane < LANES // 2, wanted, second + lax.shift_right_logical(lane, 4) - 4)
    pick = jnp.where(row == wanted, 1.0, 0.0).astype(BF)
    hits = jnp.dot(table, pick, preferred_element_type=F32)
    row = lax.broadcasted_iota(jnp.int32, hits.shape, 0)
    lane = lax.broadcasted_iota(jnp.int32, hits.shape, 1)
    owner = lax.bitwise_and(lax.shift_right_logical(row, 4) + fs, 15)
    local = lax.bitwise_and(row, SCALE_ROWS - 1)
    keep = (
        (owner == lax.bitwise_and(lane, 15))
        & (local >= group * PIECES)
        & (local < group * PIECES + PIECES)
    )
    return jnp.sum(jnp.where(keep, hits, 0.0), axis=0, keepdims=True)


def minus_expm1(x):
    series = x * (
        1.0
        + x
        * (0.5 + x * (1.0 / 6 + x * (1.0 / 24 + x * (1.0 / 120 + x * (1.0 / 720 + x / 5040)))))
    )
    return jnp.where(x > -0.5, -series, 1.0 - jnp.exp(x))


def scan_rows(factors, inputs):
    by = 1
    while by < factors.shape[0]:
        if by < 8:
            before_f, before_i = shift_rows(factors, by, 1.0), shift_rows(inputs, by, 0.0)
        else:
            top = (by, factors.shape[1])
            before_f = jnp.concatenate([jnp.ones(top, F32), factors[:-by]], axis=0)
            before_i = jnp.concatenate([jnp.zeros(top, F32), inputs[:-by]], axis=0)
        inputs = factors * before_i + inputs
        factors = factors * before_f
        by *= 2
    return inputs


def pack_kernel(branch_ref, gelu_ref, out_ref, *refs):
    narrow, wide = refs[:4], refs[4:6]
    gate_ref, value_ref, down_ref, mixer_ref, ffn_ref = refs[6:]
    rows = branch_ref.shape[0]
    mixer_ref[0:rows] = branch_ref[...].astype(BF)
    mixer_ref[rows : 2 * rows] = gelu_ref[...].astype(BF)
    small = [ref[...] for ref in narrow]
    small.append(jnp.zeros((1, LANES - sum(v.shape[1] for v in small)), F32))
    scales = jnp.concatenate([jnp.concatenate(small, axis=1), *[ref[...] for ref in wide]], axis=0)
    high = scales.astype(BF)
    rest = scales - high.astype(F32)
    middle = rest.astype(BF)
    low = (rest - middle.astype(F32)).astype(BF)
    parts = []
    for group in range(scales.shape[0]):
        for piece in (high, middle, low):
            parts.append(piece[group : group + 1].astype(F32))
    parts.append(jnp.zeros((SCALE_ROWS - len(parts), LANES), F32))
    mixer_ref[2 * rows : 2 * rows + SCALE_ROWS] = jnp.concatenate(parts, axis=0).astype(BF)
    mixer_ref[2 * rows + SCALE_ROWS :] = out_ref[...].astype(BF)

    rows, width = gate_ref.shape[1], gate_ref.shape[0]
    full = width // LANES
    for j in range(full):
        cols = slice(j * LANES, (j + 1) * LANES)
        ffn_ref[2 * j * rows : (2 * j + 1) * rows] = gate_ref[cols].T.astype(BF)
        ffn_ref[(2 * j + 1) * rows : (2 * j + 2) * rows] = value_ref[cols].T.astype(BF)
    mixed = jnp.concatenate([gate_ref[full * LANES :], value_ref[full * LANES :]], axis=0)
    ffn_ref[2 * full * rows : (2 * full + 1) * rows] = mixed.T.astype(BF)
    ffn_ref[(2 * full + 1) * rows :] = down_ref[...].astype(BF)


def mixer_kernel(pos_ref, *refs):
    tokens = refs[:8]
    (w_ref, gain_ref, taps_ref, gates_ref, rate_ref, out_ref, table_ref, x_ref, full_ref,
     scale_ref) = refs[8:]
    tp, fs = pos_ref[0], pos_ref[1]
    size = w_ref.shape[0]
    width = tokens[0].shape[1]
    per_slot = width // LANES

    @pl.when(pl.program_id(0) == 0)
    def _():
        for slot, place in enumerate(SLOTS):
            device = slot_device(tp, place)
            for part in range(per_slot):
                at = lax.rem(device * per_slot + part - fs + size, size)
                base = slot * width + part * LANES
                full_ref[base : base + LANES, :LANES] = w_ref[at, :LANES]
                full_ref[base : base + LANES, LANES:] = w_ref[at, LANES : 2 * LANES]
        table = w_ref[:, 2 * LANES : 2 * LANES + SCALE_ROWS].reshape(size * SCALE_ROWS, LANES)
        table_ref[...] = table
        scale_ref[:, :LANES] = spread_scale(table, 0, 0, fs)
        scale_ref[:, LANES:] = spread_scale(table, 0, 8, fs)

    squares = None
    for slot in range(len(SLOTS)):
        values = tokens[slot][...].astype(F32)
        square = jnp.sum(values * values, axis=-1, keepdims=True)
        squares = square if squares is None else squares + square
    inverse = lax.rsqrt(squares * (1.0 / x_ref.shape[1]) + EPS)
    for slot, place in enumerate(SLOTS):
        values = tokens[slot][...].astype(F32)
        gain = gain_ref[slot_device(tp, place)]
        x_ref[:, slot * width : (slot + 1) * width] = (values * inverse * gain).astype(BF)
    both = jnp.dot(x_ref[...], full_ref[...], preferred_element_type=F32)
    taps = taps_ref[...] * scale_ref[:, :LANES]
    convolved = causal_mix(both[:, :LANES], taps).astype(BF)
    rates = jax.nn.sigmoid(jnp.dot(convolved, gates_ref[...], preferred_element_type=F32))
    log_decay = rates[:, :LANES] * rate_ref[...]
    driven = jnp.sqrt(minus_expm1(2.0 * log_decay)) * rates[:, LANES:] * convolved.astype(F32)
    states = scan_rows(jnp.exp(log_decay), driven)
    gelu_in = both[:, LANES:] * scale_ref[:, LANES:]
    out_ref[...] = (states * jax.nn.gelu(gelu_in)).astype(BF)


def scales_kernel(pos_ref, table_ref, taps_ref, cols_ref, mixed_ref, down_ref):
    tp, fs = pos_ref[0], pos_ref[1]
    table = table_ref[...]
    per_slot = down_ref.shape[1] // LANES
    for slot, place in enumerate(SLOTS):
        device = slot_device(tp, place)
        for part in range(per_slot):
            block = device * per_slot + part
            base = (slot * per_slot + part) * LANES
            cols_ref[:, base : base + LANES] = spread_scale(table, 1, block * 8, fs)
            if slot == 0:
                down_ref[:, base : base + LANES] = spread_scale(table, 2, block * 8, fs)
    gate_at, value_at = 16, 60
    pairs = (mixed_ref.shape[1] // LANES) // 2
    for j in range(pairs):
        cols = slice(2 * j * LANES, (2 * j + 1) * LANES)
        mixed_ref[:, cols] = taps_ref[:, cols] * spread_scale(table, 0, gate_at + 8 * j, fs)
        cols = slice((2 * j + 1) * LANES, (2 * j + 2) * LANES)
        mixed_ref[:, cols] = taps_ref[:, cols] * spread_scale(table, 0, value_at + 8 * j, fs)
    cols = slice(2 * pairs * LANES, (2 * pairs + 1) * LANES)
    mixed_ref[:, cols] = taps_ref[:, cols] * spread_scale(
        table, 0, gate_at + 8 * pairs, fs, value_at + 8 * pairs
    )


def out_kernel(pos_ref, *refs):
    tokens, gated, weights = refs[:8], refs[8:10], refs[10:12]
    scale_ref, gain_ref, normed_ref, own_ref, hidden_ref = refs[12:]
    tp, fs = pos_ref[0], pos_ref[1]
    size = weights[0].shape[1] // LANES
    width = tokens[0].shape[1]
    per_slot = width // LANES

    def weight_columns(place):
        columns = []
        for part in range(per_slot):
            at = lax.rem(slot_device(tp, place) * per_slot + part - fs + size, size)
            rows = pl.ds(pl.multiple_of(at * LANES, LANES), LANES)
            blocks = [ref[k, rows] for ref in weights for k in range(HALF_SLOTS)]
            columns.append(jnp.concatenate(blocks, axis=0))
        return jnp.concatenate(columns, axis=1)

    states = jnp.concatenate([ref[k] for ref in gated for k in range(HALF_SLOTS)], axis=1)
    squares = None
    for slot, place in enumerate(SLOTS):
        cols = slice(slot * width, (slot + 1) * width)
        mixed = jnp.dot(states, weight_columns(place), preferred_element_type=F32)
        mixed = mixed * scale_ref[:, cols]
        hidden = (tokens[slot][...].astype(F32) + mixed).astype(BF)
        hidden_ref[:, cols] = hidden
        if slot == 0:
            own_ref[...] = hidden
        values = hidden.astype(F32)
        square = jnp.sum(values * values, axis=-1, keepdims=True)
        squares = square if squares is None else squares + square
    inverse = lax.rsqrt(squares * (1.0 / hidden_ref.shape[1]) + EPS)
    for slot, place in enumerate(SLOTS):
        device = slot_device(tp, place)
        values = hidden_ref[:, slot * width : (slot + 1) * width].astype(F32)
        normed_ref[device] = (values * inverse * gain_ref[device]).astype(BF)


def ffn_kernel(pos_ref, x_ref, taps_ref, w_ref, send_ref, keep_ref, hidden_ref):
    tp = pos_ref[0]
    count, rows, width = x_ref.shape
    per_slot = width // LANES
    up_rows = taps_ref.shape[1]
    pairs = (up_rows // LANES) // 2
    depth = count * width
    def columns(j):
        return w_ref[:, j * LANES : (j + 1) * LANES].reshape(depth, LANES)

    x = jnp.concatenate([x_ref[k] for k in range(count)], axis=1)
    for j in range(pairs):
        weight = jnp.concatenate([columns(2 * j), columns(2 * j + 1)], axis=1)
        both = jnp.dot(x, weight, preferred_element_type=F32)
        both = causal_mix(both, taps_ref[:, 2 * j * LANES : (2 * j + 2) * LANES])
        gate = both[:, :LANES]
        hidden_ref[:, j * LANES : (j + 1) * LANES] = (
            gate * jax.nn.sigmoid(gate) * both[:, LANES:]
        ).astype(BF)
    both = jnp.dot(x, columns(2 * pairs), preferred_element_type=F32)
    both = causal_mix(both, taps_ref[:, 2 * pairs * LANES :])
    product = both * jax.nn.sigmoid(both) * pltpu.roll(both, LANES // 2, 1)
    hidden_ref[:, pairs * LANES :] = product[:, : LANES // 2].astype(BF)
    hidden = hidden_ref[...]
    for slot, place in enumerate(SLOTS):
        device = slot_device(tp, place)
        weight = jnp.concatenate(
            [w_ref[device * per_slot + part, up_rows:] for part in range(per_slot)], axis=1
        )
        term = jnp.dot(hidden, weight, preferred_element_type=F32).astype(BF)
        target = keep_ref if slot < HALF_SLOTS else send_ref
        target[slot % HALF_SLOTS] = term


def whole(array):
    rank = array.ndim
    return pl.BlockSpec(array.shape, lambda i, pos: (0,) * rank, pipeline_mode=pl.Buffered(1))


def row_block(rows, width):
    return pl.BlockSpec((rows, width), lambda i, pos: (i, 0))


def slab(count, rows, width):
    return pl.BlockSpec((count, rows, width), lambda i, pos: (0, i, 0))


def fixed(shape):
    rank = len(shape)
    return pl.BlockSpec(shape, lambda i, pos: (0,) * rank)


def call(kernel, position, steps, operands, in_specs, outs, out_specs, scratch, flops, name):
    size = sum(a.size * a.dtype.itemsize for a in operands)
    return pl.pallas_call(
        kernel,
        grid_spec=pltpu.PrefetchScalarGridSpec(
            num_scalar_prefetch=1,
            grid=(steps,),
            in_specs=in_specs,
            out_specs=out_specs,
            scratch_shapes=scratch,
        ),
        out_shape=outs,
        compiler_params=pltpu.CompilerParams(dimension_semantics=("arbitrary",)),
        cost_estimate=pl.CostEstimate(flops=flops, transcendentals=0, bytes_accessed=size),
        name=name,
    )(position, *operands)


def add_rounded(one, other):
    return (one.astype(F32) + other.astype(F32)).astype(BF)


def block_diagonal(blocks):
    count, size, _ = blocks.shape
    rows = []
    for i in range(count):
        rows.append(jnp.pad(blocks[i], ((0, 0), (i * size, (count - 1 - i) * size))))
    return jnp.concatenate(rows, axis=0)


def per_device(
    tokens,
    mixer_gain,
    branch_weight,
    gelu_weight,
    branch_scale,
    gelu_scale,
    branch_taps,
    recur_gate,
    input_gate,
    decay_param,
    out_weight,
    out_scale,
    ffn_gain,
    upgate_weight,
    upval_weight,
    upgate_scale,
    upval_scale,
    upgate_taps,
    upval_taps,
    down_weight,
    down_scale,
):
    fs_size, tp_size = lax.axis_size("fs"), lax.axis_size("tp")
    rows, width = tokens.shape
    depth = width * tp_size
    steps = rows // SEQ_LEN
    position = jnp.stack([lax.axis_index("tp"), lax.axis_index("fs")]).astype(jnp.int32)

    hidden_width = upgate_weight.shape[1]
    up_rows = 2 * hidden_width * upgate_weight.shape[0] // LANES
    ffn_rows = up_rows + hidden_width
    front = 2 * LANES + SCALE_ROWS
    packed_mixer, packed_ffn = pl.pallas_call(
        pack_kernel,
        out_shape=(
            jax.ShapeDtypeStruct((front + LANES, LANES), BF),
            jax.ShapeDtypeStruct((ffn_rows, LANES), BF),
        ),
        name="pack",
    )(
        branch_weight,
        gelu_weight,
        out_weight,
        branch_scale,
        gelu_scale,
        upgate_scale,
        upval_scale,
        out_scale,
        down_scale,
        upgate_weight.T,
        upval_weight.T,
        down_weight,
    )
    ffn_weights = lax.all_gather(packed_ffn, "fs", axis=0, tiled=True)
    ffn_weights = ffn_weights.reshape(fs_size, ffn_rows, LANES)

    tokens, packed_mixer = lax.optimization_barrier((tokens, packed_mixer))
    token_slots = gather_directly(tokens)
    pieces = ring_fs(packed_mixer, 208)
    out_rows = pieces[:, front:].reshape(fs_size * LANES, LANES)
    out_right, out_left = near_chips(out_rows)

    gates = jnp.concatenate([block_diagonal(recur_gate), block_diagonal(input_gate)], axis=1)
    rate = (-8.0 * jax.nn.softplus(-decay_param))[None]
    mixer_gains = mixer_gain.reshape(tp_size, 1, width)
    ffn_gains = ffn_gain.reshape(tp_size, 1, width)
    token_specs = [row_block(SEQ_LEN, width)] * len(SLOTS)

    tail = (pieces, mixer_gains, branch_taps, gates, rate)
    table_shape = (fs_size * SCALE_ROWS, LANES)
    gated, table = call(
        mixer_kernel,
        position,
        steps,
        (*token_slots, *tail),
        token_specs + [whole(a) for a in tail],
        (jax.ShapeDtypeStruct((rows, LANES), BF), jax.ShapeDtypeStruct(table_shape, BF)),
        (row_block(SEQ_LEN, LANES), fixed(table_shape)),
        [
            pltpu.VMEM((SEQ_LEN, depth), BF),
            pltpu.VMEM((depth, 2 * LANES), BF),
            pltpu.VMEM((1, 2 * LANES), F32),
        ],
        2 * rows * depth * 2 * LANES,
        "mixer",
    )
    near = lax.optimization_barrier((out_right, out_left, *near_chips(gated)))
    far = lax.optimization_barrier((*far_chip(*near[2:]), *far_chip(*near[:2])))
    gated_slots = complete_tp(gated, *near[2:], far[:2])
    out_slots = complete_tp(out_rows, *near[:2], far[2:])

    edge = hidden_width // LANES * LANES
    tap_parts = []
    for j in range(hidden_width // LANES):
        tap_parts += [upgate_taps[:, j * LANES : (j + 1) * LANES]]
        tap_parts += [upval_taps[:, j * LANES : (j + 1) * LANES]]
    tap_parts += [upgate_taps[:, edge:], upval_taps[:, edge:]]
    ffn_taps = jnp.concatenate(tap_parts, axis=1)
    vmem = pl.BlockSpec(memory_space=pltpu.VMEM)
    out_cols, scaled_taps, down_cols = pl.pallas_call(
        scales_kernel,
        in_specs=[pl.BlockSpec(memory_space=pltpu.SMEM), vmem, vmem],
        out_specs=(vmem, vmem, vmem),
        out_shape=(
            jax.ShapeDtypeStruct((1, depth), F32),
            jax.ShapeDtypeStruct(ffn_taps.shape, F32),
            jax.ShapeDtypeStruct((1, width), F32),
        ),
        name="spread_scales",
    )(position, table, ffn_taps)

    block = SEQ_LEN // 2
    tail = (out_cols, ffn_gains)
    normed, own_hidden = call(
        out_kernel,
        position,
        rows // block,
        (*token_slots, *gated_slots, *out_slots, *tail),
        [row_block(block, width)] * len(SLOTS)
        + [slab(HALF_SLOTS, block, LANES)] * CORES
        + [whole(a) for a in (*out_slots, *tail)],
        (
            jax.ShapeDtypeStruct((tp_size, rows, width), BF),
            jax.ShapeDtypeStruct((rows, width), BF),
        ),
        (slab(tp_size, block, width), row_block(block, width)),
        [pltpu.VMEM((block, depth), BF)],
        2 * rows * tp_size * LANES * depth,
        "out_proj",
    )

    term = jax.ShapeDtypeStruct((HALF_SLOTS, rows, width), BF)
    send, keep = call(
        ffn_kernel,
        position,
        steps,
        (normed, scaled_taps, ffn_weights),
        [slab(tp_size, SEQ_LEN, width), whole(scaled_taps), whole(ffn_weights)],
        (term, term),
        (slab(HALF_SLOTS, SEQ_LEN, width), slab(HALF_SLOTS, SEQ_LEN, width)),
        [pltpu.VMEM((SEQ_LEN, hidden_width), BF)],
        6 * rows * depth * hidden_width,
        "ffn",
    )
    received = from_partner(send)

    def added(slot, low, high):
        both = keep[slot, low:high].astype(F32) + received[slot, low:high].astype(F32)
        return both.astype(BF)

    half = rows // 2
    via_right = from_chip(added(2, 0, half), -1)
    via_left = from_chip(added(2, half, rows), 1)
    left_bottom = from_chip(added(1, half, rows), -1)
    right_top = from_chip(added(3, 0, half), 1)
    left_top = from_chip(add_rounded(added(1, 0, half), via_right), -1)
    right_bottom = from_chip(add_rounded(added(3, half, rows), via_left), 1)
    left_sum = jnp.concatenate([left_top, left_bottom], axis=0).astype(F32)
    right_sum = jnp.concatenate([right_top, right_bottom], axis=0).astype(F32)
    total = added(0, 0, rows).astype(F32) + left_sum + right_sum
    return (own_hidden.astype(F32) + total * down_cols).astype(BF)


def solution(mesh):
    in_specs = (
        P(("grp", "fs"), "tp"),
        P(),
        P("fs", "tp"),
        P("fs", "tp"),
        P("fs", "tp"),
        P("fs", "tp"),
        P(None, "tp"),
        P("tp", None, None),
        P("tp", None, None),
        P("tp"),
        P("tp", "fs"),
        P("fs", None),
        P(),
        P("fs", "tp"),
        P("fs", "tp"),
        P("fs", "tp"),
        P("fs", "tp"),
        P(None, "tp"),
        P(None, "tp"),
        P("tp", "fs"),
        P("fs", None),
    )
    out_specs = P(("grp", "fs"), "tp")
    return jax.shard_map(
        per_device, mesh=mesh, in_specs=in_specs, out_specs=out_specs, check_vma=False
    )
```

```python
import jax
import jax.numpy as jnp
from jax import lax
from jax.experimental import pallas as pl
from jax.experimental.pallas import tpu as pltpu
from jax.sharding import PartitionSpec as P


SEQ_LEN = 512
EPS = 1e-06
BF = jnp.bfloat16
F32 = jnp.float32
LANES = 128
CORES = 2
SLOTS = ((0, 0), (1, 0), (2, 0), (3, 0), (0, 1), (1, 1), (2, 1), (3, 1))
HALF_SLOTS = 4
SCALE_ROWS = 16
PIECES = 3


def from_chip(value, step):
    size = lax.axis_size("tp")
    chips = size // CORES
    pairs = [(i, ((i // CORES - step) % chips) * CORES + i % CORES) for i in range(size)]
    return lax.ppermute(value, "tp", pairs)


def from_partner(value):
    size = lax.axis_size("tp")
    return lax.ppermute(value, "tp", [(i, i ^ 1) for i in range(size)])


def near_chips(value):
    return from_chip(value, 1), from_chip(value, -1)


def far_chip(right, left):
    half = right.shape[0] // 2
    return from_chip(right[:half], 1), from_chip(left[half:], -1)


def complete_tp(value, right, left, far):
    same = jnp.stack([value, right, jnp.concatenate(far, axis=0), left])
    return same, from_partner(same)


def gather_directly(value):
    size = lax.axis_size("tp")
    chips = size // CORES
    slots = [value]
    for step, other in SLOTS[1:]:
        pairs = [
            (i, ((i // CORES - step) % chips) * CORES + (i % CORES) ^ other) for i in range(size)
        ]
        slots.append(lax.ppermute(value, "tp", pairs))
    return slots


def ring_fs(halves):
    size, groups = lax.axis_size("fs"), lax.axis_size("grp")
    rounds = size // 4
    beside = [(i, i ^ 1) for i in range(groups)]
    mine = lax.rem(lax.axis_index("grp"), 2)
    own = lax.dynamic_index_in_dim(halves, mine, 0, keepdims=False)
    other = lax.dynamic_index_in_dim(halves, 1 - mine, 0, keepdims=False)
    stack = jnp.zeros((2, rounds + 1, 4, *own.shape), own.dtype)
    stack = lax.dynamic_update_slice(stack, own[None, None, None], (0, 0, 1, 0, 0))
    stack = lax.dynamic_update_slice(stack, other[None, None, None], (1, 0, 1, 0, 0))

    def from_place(value, step):
        return lax.ppermute(value, "fs", [(i, (i - step) % size) for i in range(size)])

    def further(above, below):
        return (
            from_place(above, 1),
            from_place(above, 2),
            from_place(below, -1),
            from_place(below, -2),
        )

    def held(stack, k, arrived):
        pieces = jnp.stack(arrived)
        stack = lax.dynamic_update_slice(stack, pieces[None, None], (0, k, 0, 0, 0))
        pieces = lax.ppermute(pieces, "grp", beside)
        return lax.dynamic_update_slice(stack, pieces[None, None], (1, k, 0, 0, 0))

    def step(k, state):
        stack, arrived = state
        following = further(arrived[1], arrived[3])
        return held(stack, k, arrived), following

    first = further(own, own)
    stack, arrived = lax.fori_loop(1, rounds, step, (stack, first))
    return held(stack, rounds, arrived)


def slot_device(tp, slot):
    step, other = slot
    core = lax.rem(tp, CORES)
    chip = lax.rem(lax.div(tp, CORES) + step + HALF_SLOTS, HALF_SLOTS)
    return chip * CORES + (1 - core if other else core)


def shift_rows(values, by, fill):
    rows = lax.broadcasted_iota(jnp.int32, values.shape, 0)
    return jnp.where(rows >= by, pltpu.roll(values, by, 0), fill)


def causal_mix(values, taps):
    count = taps.shape[0]
    total = values * taps[count - 1 : count]
    for by in range(1, count):
        total = total + shift_rows(values, by, 0.0) * taps[count - 1 - by : count - by]
    return total


def spread_scale(table, group, first, second=None):
    shape = (LANES, LANES)
    lane = lax.broadcasted_iota(jnp.int32, shape, 1)
    row = lax.broadcasted_iota(jnp.int32, shape, 0)
    wanted = first + lax.shift_right_logical(lane, 4)
    if second is not None:
        wanted = jnp.where(lane < LANES // 2, wanted, second + lax.shift_right_logical(lane, 4) - 4)
    pick = jnp.where(row == wanted, 1.0, 0.0).astype(BF)
    hits = jnp.dot(table, pick, preferred_element_type=F32)
    row = lax.broadcasted_iota(jnp.int32, hits.shape, 0)
    lane = lax.broadcasted_iota(jnp.int32, hits.shape, 1)
    owner = lax.shift_right_logical(row, 4)
    local = lax.bitwise_and(row, SCALE_ROWS - 1)
    keep = (
        (owner == lax.bitwise_and(lane, 15))
        & (local >= group * PIECES)
        & (local < group * PIECES + PIECES)
    )
    return jnp.sum(jnp.where(keep, hits, 0.0), axis=0, keepdims=True)


def minus_expm1(x):
    series = x * (
        1.0
        + x
        * (0.5 + x * (1.0 / 6 + x * (1.0 / 24 + x * (1.0 / 120 + x * (1.0 / 720 + x / 5040)))))
    )
    return jnp.where(x > -0.5, -series, 1.0 - jnp.exp(x))


def scan_rows(factors, inputs):
    by = 1
    while by < factors.shape[0]:
        if by < 8:
            before_f, before_i = shift_rows(factors, by, 1.0), shift_rows(inputs, by, 0.0)
        else:
            top = (by, factors.shape[1])
            before_f = jnp.concatenate([jnp.ones(top, F32), factors[:-by]], axis=0)
            before_i = jnp.concatenate([jnp.zeros(top, F32), inputs[:-by]], axis=0)
        inputs = factors * before_i + inputs
        factors = factors * before_f
        by *= 2
    return inputs


def pack_kernel(branch_ref, gelu_ref, out_ref, *refs):
    narrow, wide = refs[:4], refs[4:6]
    gate_ref, value_ref, down_ref, mixer_ref, ffn_ref = refs[6:]
    rows = branch_ref.shape[0]
    cut = rows + SCALE_ROWS
    mixer_ref[0, 0:rows] = branch_ref[...].astype(BF)
    mixer_ref[1, 0:rows] = gelu_ref[...].astype(BF)
    mixer_ref[0, cut:] = out_ref[: rows // 2].astype(BF)
    mixer_ref[1, cut:] = out_ref[rows // 2 :].astype(BF)
    small = [ref[...] for ref in narrow]
    small.append(jnp.zeros((1, LANES - sum(v.shape[1] for v in small)), F32))
    scales = jnp.concatenate([jnp.concatenate(small, axis=1), *[ref[...] for ref in wide]], axis=0)
    high = scales.astype(BF)
    rest = scales - high.astype(F32)
    middle = rest.astype(BF)
    low = (rest - middle.astype(F32)).astype(BF)
    parts = []
    for group in range(scales.shape[0]):
        for piece in (high, middle, low):
            parts.append(piece[group : group + 1].astype(F32))
    parts.append(jnp.zeros((SCALE_ROWS - len(parts), LANES), F32))
    packed = jnp.concatenate(parts, axis=0).astype(BF)
    mixer_ref[0, rows:cut] = packed
    mixer_ref[1, rows:cut] = packed

    rows, width = gate_ref.shape[1], gate_ref.shape[0]
    full = width // LANES
    for j in range(full):
        cols = slice(j * LANES, (j + 1) * LANES)
        ffn_ref[2 * j * rows : (2 * j + 1) * rows] = gate_ref[cols].T.astype(BF)
        ffn_ref[(2 * j + 1) * rows : (2 * j + 2) * rows] = value_ref[cols].T.astype(BF)
    mixed = jnp.concatenate([gate_ref[full * LANES :], value_ref[full * LANES :]], axis=0)
    ffn_ref[2 * full * rows : (2 * full + 1) * rows] = mixed.T.astype(BF)
    ffn_ref[(2 * full + 1) * rows :] = down_ref[...].astype(BF)


def unpack_kernel(pos_ref, stack_ref, weight_ref, table_ref, out_ref):
    fs, mine = pos_ref[1], pos_ref[2]
    size = weight_ref.shape[0]
    cut = LANES + SCALE_ROWS
    for block in range(size):
        at = lax.rem(block - fs + size, size)
        below = at > size // 2
        places = jnp.where(below, size - at, at)
        k = lax.div(places + 1, 2)
        side = jnp.where(below, 3, 1) - lax.rem(places, 2)
        rows = block * LANES
        for half in range(2):
            piece = stack_ref.at[jnp.where(mine == half, 0, 1), k, side]
            weight_ref[block, :, half * LANES : (half + 1) * LANES] = piece[:LANES]
            out_ref[rows : rows + LANES // 2] = piece[cut:]
            rows += LANES // 2
            if half == 0:
                table_ref[block * SCALE_ROWS : (block + 1) * SCALE_ROWS] = piece[LANES:cut]


def mixer_kernel(pos_ref, *refs):
    tokens = refs[:8]
    (w_ref, table_ref, gain_ref, taps_ref, gates_ref, rate_ref, out_ref, x_ref, full_ref,
     scale_ref) = refs[8:]
    tp = pos_ref[0]
    width = tokens[0].shape[1]
    per_slot = width // LANES

    @pl.when(pl.program_id(0) == 0)
    def _():
        for slot, place in enumerate(SLOTS):
            device = slot_device(tp, place)
            for part in range(per_slot):
                base = slot * width + part * LANES
                full_ref[base : base + LANES] = w_ref[device * per_slot + part]
        table = table_ref[...]
        scale_ref[:, :LANES] = spread_scale(table, 0, 0)
        scale_ref[:, LANES:] = spread_scale(table, 0, 8)

    squares = None
    for slot in range(len(SLOTS)):
        values = tokens[slot][...].astype(F32)
        square = jnp.sum(values * values, axis=-1, keepdims=True)
        squares = square if squares is None else squares + square
    inverse = lax.rsqrt(squares * (1.0 / x_ref.shape[1]) + EPS)
    for slot, place in enumerate(SLOTS):
        values = tokens[slot][...].astype(F32)
        gain = gain_ref[slot_device(tp, place)]
        x_ref[:, slot * width : (slot + 1) * width] = (values * inverse * gain).astype(BF)
    both = jnp.dot(x_ref[...], full_ref[...], preferred_element_type=F32)
    taps = taps_ref[...] * scale_ref[:, :LANES]
    convolved = causal_mix(both[:, :LANES], taps).astype(BF)
    rates = jax.nn.sigmoid(jnp.dot(convolved, gates_ref[...], preferred_element_type=F32))
    log_decay = rates[:, :LANES] * rate_ref[...]
    driven = jnp.sqrt(minus_expm1(2.0 * log_decay)) * rates[:, LANES:] * convolved.astype(F32)
    states = scan_rows(jnp.exp(log_decay), driven)
    gelu_in = both[:, LANES:] * scale_ref[:, LANES:]
    out_ref[...] = (states * jax.nn.gelu(gelu_in)).astype(BF)


def scales_kernel(pos_ref, table_ref, taps_ref, cols_ref, mixed_ref, down_ref):
    tp = pos_ref[0]
    table = table_ref[...]
    per_slot = down_ref.shape[1] // LANES
    for slot, place in enumerate(SLOTS):
        device = slot_device(tp, place)
        for part in range(per_slot):
            block = device * per_slot + part
            base = (slot * per_slot + part) * LANES
            cols_ref[:, base : base + LANES] = spread_scale(table, 1, block * 8)
            if slot == 0:
                down_ref[:, base : base + LANES] = spread_scale(table, 2, block * 8)
    gate_at, value_at = 16, 60
    pairs = (mixed_ref.shape[1] // LANES) // 2
    for j in range(pairs):
        cols = slice(2 * j * LANES, (2 * j + 1) * LANES)
        mixed_ref[:, cols] = taps_ref[:, cols] * spread_scale(table, 0, gate_at + 8 * j)
        cols = slice((2 * j + 1) * LANES, (2 * j + 2) * LANES)
        mixed_ref[:, cols] = taps_ref[:, cols] * spread_scale(table, 0, value_at + 8 * j)
    cols = slice(2 * pairs * LANES, (2 * pairs + 1) * LANES)
    mixed_ref[:, cols] = taps_ref[:, cols] * spread_scale(
        table, 0, gate_at + 8 * pairs, value_at + 8 * pairs
    )


def out_kernel(pos_ref, *refs):
    tokens, gated, weights = refs[:8], refs[8:10], refs[10:12]
    scale_ref, gain_ref, normed_ref, own_ref, hidden_ref = refs[12:]
    tp = pos_ref[0]
    width = tokens[0].shape[1]
    per_slot = width // LANES

    def weight_columns(place):
        columns = []
        for part in range(per_slot):
            at = slot_device(tp, place) * per_slot + part
            rows = pl.ds(pl.multiple_of(at * LANES, LANES), LANES)
            blocks = [ref[k, rows] for ref in weights for k in range(HALF_SLOTS)]
            columns.append(jnp.concatenate(blocks, axis=0))
        return jnp.concatenate(columns, axis=1)

    states = jnp.concatenate([ref[k] for ref in gated for k in range(HALF_SLOTS)], axis=1)
    squares = None
    for slot, place in enumerate(SLOTS):
        cols = slice(slot * width, (slot + 1) * width)
        mixed = jnp.dot(states, weight_columns(place), preferred_element_type=F32)
        mixed = mixed * scale_ref[:, cols]
        hidden = (tokens[slot][...].astype(F32) + mixed).astype(BF)
        hidden_ref[:, cols] = hidden
        if slot == 0:
            own_ref[...] = hidden
        values = hidden.astype(F32)
        square = jnp.sum(values * values, axis=-1, keepdims=True)
        squares = square if squares is None else squares + square
    inverse = lax.rsqrt(squares * (1.0 / hidden_ref.shape[1]) + EPS)
    for slot, place in enumerate(SLOTS):
        device = slot_device(tp, place)
        values = hidden_ref[:, slot * width : (slot + 1) * width].astype(F32)
        normed_ref[device] = (values * inverse * gain_ref[device]).astype(BF)


def ffn_kernel(pos_ref, x_ref, taps_ref, w_ref, send_ref, keep_ref, hidden_ref):
    tp = pos_ref[0]
    count, _, width = x_ref.shape
    per_slot = width // LANES
    up_rows = taps_ref.shape[1]
    pairs = (up_rows // LANES) // 2
    depth = count * width

    def columns(j):
        return w_ref[:, j * LANES : (j + 1) * LANES].reshape(depth, LANES)

    x = jnp.concatenate([x_ref[k] for k in range(count)], axis=1)
    for j in range(pairs):
        weight = jnp.concatenate([columns(2 * j), columns(2 * j + 1)], axis=1)
        both = jnp.dot(x, weight, preferred_element_type=F32)
        both = causal_mix(both, taps_ref[:, 2 * j * LANES : (2 * j + 2) * LANES])
        gate = both[:, :LANES]
        hidden_ref[:, j * LANES : (j + 1) * LANES] = (
            gate * jax.nn.sigmoid(gate) * both[:, LANES:]
        ).astype(BF)
    both = jnp.dot(x, columns(2 * pairs), preferred_element_type=F32)
    both = causal_mix(both, taps_ref[:, 2 * pairs * LANES :])
    product = both * jax.nn.sigmoid(both) * pltpu.roll(both, LANES // 2, 1)
    hidden_ref[:, pairs * LANES :] = product[:, : LANES // 2].astype(BF)
    hidden = hidden_ref[...]
    for slot, place in enumerate(SLOTS):
        device = slot_device(tp, place)
        weight = jnp.concatenate(
            [w_ref[device * per_slot + part, up_rows:] for part in range(per_slot)], axis=1
        )
        term = jnp.dot(hidden, weight, preferred_element_type=F32).astype(BF)
        target = keep_ref if slot < HALF_SLOTS else send_ref
        target[slot % HALF_SLOTS] = term


def whole(array):
    rank = array.ndim
    return pl.BlockSpec(array.shape, lambda i, pos: (0,) * rank, pipeline_mode=pl.Buffered(1))


def row_block(rows, width):
    return pl.BlockSpec((rows, width), lambda i, pos: (i, 0))


def slab(count, rows, width):
    return pl.BlockSpec((count, rows, width), lambda i, pos: (0, i, 0))


def call(kernel, position, steps, operands, in_specs, outs, out_specs, scratch, flops):
    size = sum(a.size * a.dtype.itemsize for a in operands)
    return pl.pallas_call(
        kernel,
        grid_spec=pltpu.PrefetchScalarGridSpec(
            num_scalar_prefetch=1,
            grid=(steps,),
            in_specs=in_specs,
            out_specs=out_specs,
            scratch_shapes=scratch,
        ),
        out_shape=outs,
        compiler_params=pltpu.CompilerParams(dimension_semantics=("arbitrary",)),
        cost_estimate=pl.CostEstimate(flops=flops, transcendentals=0, bytes_accessed=size),
    )(position, *operands)


def add_rounded(one, other):
    return (one.astype(F32) + other.astype(F32)).astype(BF)


def block_diagonal(blocks):
    count, size, _ = blocks.shape
    rows = []
    for i in range(count):
        rows.append(jnp.pad(blocks[i], ((0, 0), (i * size, (count - 1 - i) * size))))
    return jnp.concatenate(rows, axis=0)


def per_device(
    tokens,
    mixer_gain,
    branch_weight,
    gelu_weight,
    branch_scale,
    gelu_scale,
    branch_taps,
    recur_gate,
    input_gate,
    decay_param,
    out_weight,
    out_scale,
    ffn_gain,
    upgate_weight,
    upval_weight,
    upgate_scale,
    upval_scale,
    upgate_taps,
    upval_taps,
    down_weight,
    down_scale,
):
    fs_size, tp_size = lax.axis_size("fs"), lax.axis_size("tp")
    rows, width = tokens.shape
    depth = width * tp_size
    steps = rows // SEQ_LEN
    mine = lax.rem(lax.axis_index("grp"), 2)
    position = jnp.stack([lax.axis_index("tp"), lax.axis_index("fs"), mine]).astype(jnp.int32)

    hidden_width = upgate_weight.shape[1]
    up_rows = 2 * hidden_width * upgate_weight.shape[0] // LANES
    ffn_rows = up_rows + hidden_width
    half_rows = LANES + SCALE_ROWS + LANES // 2
    packed_mixer, packed_ffn = pl.pallas_call(
        pack_kernel,
        out_shape=(
            jax.ShapeDtypeStruct((2, half_rows, LANES), BF),
            jax.ShapeDtypeStruct((ffn_rows, LANES), BF),
        ),
        name="pack",
    )(
        branch_weight,
        gelu_weight,
        out_weight,
        branch_scale,
        gelu_scale,
        upgate_scale,
        upval_scale,
        out_scale,
        down_scale,
        upgate_weight.T,
        upval_weight.T,
        down_weight,
    )
    ffn_weights = lax.all_gather(packed_ffn, "fs", axis=0, tiled=True)
    ffn_weights = ffn_weights.reshape(fs_size, ffn_rows, LANES)

    tokens, packed_mixer = lax.optimization_barrier((tokens, packed_mixer))
    token_slots = gather_directly(tokens)
    smem = pl.BlockSpec(memory_space=pltpu.SMEM)
    vmem = pl.BlockSpec(memory_space=pltpu.VMEM)
    mixer_weights, table, out_rows = pl.pallas_call(
        unpack_kernel,
        in_specs=[smem, vmem],
        out_specs=(vmem, vmem, vmem),
        out_shape=(
            jax.ShapeDtypeStruct((fs_size, LANES, 2 * LANES), BF),
            jax.ShapeDtypeStruct((fs_size * SCALE_ROWS, LANES), BF),
            jax.ShapeDtypeStruct((fs_size * LANES, LANES), BF),
        ),
        name="unpack",
    )(position, ring_fs(packed_mixer))
    out_right, out_left = near_chips(out_rows)

    gates = jnp.concatenate([block_diagonal(recur_gate), block_diagonal(input_gate)], axis=1)
    rate = (-8.0 * jax.nn.softplus(-decay_param))[None]
    mixer_gains = mixer_gain.reshape(tp_size, 1, width)
    ffn_gains = ffn_gain.reshape(tp_size, 1, width)
    token_specs = [row_block(SEQ_LEN, width)] * len(SLOTS)

    tail = (mixer_weights, table, mixer_gains, branch_taps, gates, rate)
    gated = call(
        mixer_kernel,
        position,
        steps,
        (*token_slots, *tail),
        token_specs + [whole(a) for a in tail],
        jax.ShapeDtypeStruct((rows, LANES), BF),
        row_block(SEQ_LEN, LANES),
        [
            pltpu.VMEM((SEQ_LEN, depth), BF),
            pltpu.VMEM((depth, 2 * LANES), BF),
            pltpu.VMEM((1, 2 * LANES), F32),
        ],
        2 * rows * depth * 2 * LANES,
    )
    near = lax.optimization_barrier((out_right, out_left, *near_chips(gated)))
    far = lax.optimization_barrier((*far_chip(*near[2:]), *far_chip(*near[:2])))
    gated_slots = complete_tp(gated, *near[2:], far[:2])
    out_slots = complete_tp(out_rows, *near[:2], far[2:])

    edge = hidden_width // LANES * LANES
    tap_parts = []
    for j in range(hidden_width // LANES):
        tap_parts += [upgate_taps[:, j * LANES : (j + 1) * LANES]]
        tap_parts += [upval_taps[:, j * LANES : (j + 1) * LANES]]
    tap_parts += [upgate_taps[:, edge:], upval_taps[:, edge:]]
    ffn_taps = jnp.concatenate(tap_parts, axis=1)
    out_cols, scaled_taps, down_cols = pl.pallas_call(
        scales_kernel,
        in_specs=[smem, vmem, vmem],
        out_specs=(vmem, vmem, vmem),
        out_shape=(
            jax.ShapeDtypeStruct((1, depth), F32),
            jax.ShapeDtypeStruct(ffn_taps.shape, F32),
            jax.ShapeDtypeStruct((1, width), F32),
        ),
        name="spread_scales",
    )(position, table, ffn_taps)

    block = SEQ_LEN // 2
    tail = (out_cols, ffn_gains)
    normed, own_hidden = call(
        out_kernel,
        position,
        rows // block,
        (*token_slots, *gated_slots, *out_slots, *tail),
        [row_block(block, width)] * len(SLOTS)
        + [slab(HALF_SLOTS, block, LANES)] * CORES
        + [whole(a) for a in (*out_slots, *tail)],
        (
            jax.ShapeDtypeStruct((tp_size, rows, width), BF),
            jax.ShapeDtypeStruct((rows, width), BF),
        ),
        (slab(tp_size, block, width), row_block(block, width)),
        [pltpu.VMEM((block, depth), BF)],
        2 * rows * tp_size * LANES * depth,
    )

    term = jax.ShapeDtypeStruct((HALF_SLOTS, rows, width), BF)
    send, keep = call(
        ffn_kernel,
        position,
        steps,
        (normed, scaled_taps, ffn_weights),
        [slab(tp_size, SEQ_LEN, width), whole(scaled_taps), whole(ffn_weights)],
        (term, term),
        (slab(HALF_SLOTS, SEQ_LEN, width), slab(HALF_SLOTS, SEQ_LEN, width)),
        [pltpu.VMEM((SEQ_LEN, hidden_width), BF)],
        6 * rows * depth * hidden_width,
    )
    received = from_partner(send)

    def added(slot, low, high):
        both = keep[slot, low:high].astype(F32) + received[slot, low:high].astype(F32)
        return both.astype(BF)

    half = rows // 2
    via_right = from_chip(added(2, 0, half), -1)
    via_left = from_chip(added(2, half, rows), 1)
    left_bottom = from_chip(added(1, half, rows), -1)
    right_top = from_chip(added(3, 0, half), 1)
    left_top = from_chip(add_rounded(added(1, 0, half), via_right), -1)
    right_bottom = from_chip(add_rounded(added(3, half, rows), via_left), 1)
    left_sum = jnp.concatenate([left_top, left_bottom], axis=0).astype(F32)
    right_sum = jnp.concatenate([right_top, right_bottom], axis=0).astype(F32)
    total = added(0, 0, rows).astype(F32) + left_sum + right_sum
    return (own_hidden.astype(F32) + total * down_cols).astype(BF)


def solution(mesh):
    in_specs = (
        P(("grp", "fs"), "tp"),
        P(),
        P("fs", "tp"),
        P("fs", "tp"),
        P("fs", "tp"),
        P("fs", "tp"),
        P(None, "tp"),
        P("tp", None, None),
        P("tp", None, None),
        P("tp"),
        P("tp", "fs"),
        P("fs", None),
        P(),
        P("fs", "tp"),
        P("fs", "tp"),
        P("fs", "tp"),
        P("fs", "tp"),
        P(None, "tp"),
        P(None, "tp"),
        P("tp", "fs"),
        P("fs", None),
    )
    out_specs = P(("grp", "fs"), "tp")

    return jax.shard_map(
        per_device, mesh=mesh, in_specs=in_specs, out_specs=out_specs, check_vma=False
    )
```

```python
import jax
import jax.numpy as jnp
from jax import lax
from jax.experimental import pallas as pl
from jax.experimental.pallas import tpu as pltpu
from jax.sharding import PartitionSpec as P


SEQ_LEN = 512
EPS = 1e-06
BF = jnp.bfloat16
F32 = jnp.float32
LANES = 128
CORES = 2
SLOTS = ((0, 0), (1, 0), (2, 0), (3, 0), (0, 1), (1, 1), (2, 1), (3, 1))
HALF_SLOTS = 4
SCALE_ROWS = 16
PIECES = 3


def from_chip(value, step):
    size = lax.axis_size("tp")
    chips = size // CORES
    pairs = [(i, ((i // CORES - step) % chips) * CORES + i % CORES) for i in range(size)]
    return lax.ppermute(value, "tp", pairs)


def from_partner(value):
    size = lax.axis_size("tp")
    return lax.ppermute(value, "tp", [(i, i ^ 1) for i in range(size)])


def near_chips(value):
    return from_chip(value, 1), from_chip(value, -1)


def gather_directly(value):
    size = lax.axis_size("tp")
    chips = size // CORES
    slots = [value]
    for step, other in SLOTS[1:]:
        pairs = [
            (i, ((i // CORES - step) % chips) * CORES + (i % CORES) ^ other) for i in range(size)
        ]
        slots.append(lax.ppermute(value, "tp", pairs))
    return slots


def ring_fs(halves):
    size, groups = lax.axis_size("fs"), lax.axis_size("grp")
    rounds = size // 4
    beside = [(i, i ^ 1) for i in range(groups)]
    mine = lax.rem(lax.axis_index("grp"), 2)
    own = lax.dynamic_index_in_dim(halves, mine, 0, keepdims=False)
    other = lax.dynamic_index_in_dim(halves, 1 - mine, 0, keepdims=False)
    stack = jnp.zeros((2, rounds + 1, 4, *own.shape), own.dtype)
    stack = lax.dynamic_update_slice(stack, own[None, None, None], (0, 0, 1, 0, 0))
    stack = lax.dynamic_update_slice(stack, other[None, None, None], (1, 0, 1, 0, 0))

    def from_place(value, step):
        return lax.ppermute(value, "fs", [(i, (i - step) % size) for i in range(size)])

    def further(above, below):
        return (
            from_place(above, 1),
            from_place(above, 2),
            from_place(below, -1),
            from_place(below, -2),
        )

    def held(stack, k, arrived):
        pieces = jnp.stack(arrived)
        stack = lax.dynamic_update_slice(stack, pieces[None, None], (0, k, 0, 0, 0))
        pieces = lax.ppermute(pieces, "grp", beside)
        return lax.dynamic_update_slice(stack, pieces[None, None], (1, k, 0, 0, 0))

    def step(k, state):
        stack, arrived = state
        following = further(arrived[1], arrived[3])
        return held(stack, k, arrived), following

    first = further(own, own)
    stack, arrived = lax.fori_loop(1, rounds, step, (stack, first))
    return held(stack, rounds, arrived)


def slot_device(tp, slot):
    step, other = slot
    core = lax.rem(tp, CORES)
    chip = lax.rem(lax.div(tp, CORES) + step + HALF_SLOTS, HALF_SLOTS)
    return chip * CORES + (1 - core if other else core)


def shift_rows(values, by, fill):
    rows = lax.broadcasted_iota(jnp.int32, values.shape, 0)
    return jnp.where(rows >= by, pltpu.roll(values, by, 0), fill)


def causal_mix(values, taps):
    count = taps.shape[0]
    total = values * taps[count - 1 : count]
    for by in range(1, count):
        total = total + shift_rows(values, by, 0.0) * taps[count - 1 - by : count - by]
    return total


def spread_scale(table, group, first, second=None):
    shape = (LANES, LANES)
    lane = lax.broadcasted_iota(jnp.int32, shape, 1)
    row = lax.broadcasted_iota(jnp.int32, shape, 0)
    wanted = first + lax.shift_right_logical(lane, 4)
    if second is not None:
        wanted = jnp.where(lane < LANES // 2, wanted, second + lax.shift_right_logical(lane, 4) - 4)
    pick = jnp.where(row == wanted, 1.0, 0.0).astype(BF)
    hits = jnp.dot(table, pick, preferred_element_type=F32)
    row = lax.broadcasted_iota(jnp.int32, hits.shape, 0)
    lane = lax.broadcasted_iota(jnp.int32, hits.shape, 1)
    owner = lax.shift_right_logical(row, 4)
    local = lax.bitwise_and(row, SCALE_ROWS - 1)
    keep = (
        (owner == lax.bitwise_and(lane, 15))
        & (local >= group * PIECES)
        & (local < group * PIECES + PIECES)
    )
    return jnp.sum(jnp.where(keep, hits, 0.0), axis=0, keepdims=True)


def minus_expm1(x):
    series = x * (
        1.0
        + x
        * (0.5 + x * (1.0 / 6 + x * (1.0 / 24 + x * (1.0 / 120 + x * (1.0 / 720 + x / 5040)))))
    )
    return jnp.where(x > -0.5, -series, 1.0 - jnp.exp(x))


def scan_rows(factors, inputs):
    by = 1
    while by < factors.shape[0]:
        if by < 8:
            before_f, before_i = shift_rows(factors, by, 1.0), shift_rows(inputs, by, 0.0)
        else:
            top = (by, factors.shape[1])
            before_f = jnp.concatenate([jnp.ones(top, F32), factors[:-by]], axis=0)
            before_i = jnp.concatenate([jnp.zeros(top, F32), inputs[:-by]], axis=0)
        inputs = factors * before_i + inputs
        factors = factors * before_f
        by *= 2
    return inputs


def pack_kernel(branch_ref, gelu_ref, out_ref, *refs):
    narrow, wide = refs[:4], refs[4:6]
    gate_ref, value_ref, down_ref, mixer_ref, ffn_ref = refs[6:]
    rows = branch_ref.shape[0]
    cut = rows + SCALE_ROWS
    mixer_ref[0, 0:rows] = branch_ref[...].astype(BF)
    mixer_ref[1, 0:rows] = gelu_ref[...].astype(BF)
    mixer_ref[0, cut:] = out_ref[: rows // 2].astype(BF)
    mixer_ref[1, cut:] = out_ref[rows // 2 :].astype(BF)
    small = [ref[...] for ref in narrow]
    small.append(jnp.zeros((1, LANES - sum(v.shape[1] for v in small)), F32))
    scales = jnp.concatenate([jnp.concatenate(small, axis=1), *[ref[...] for ref in wide]], axis=0)
    high = scales.astype(BF)
    rest = scales - high.astype(F32)
    middle = rest.astype(BF)
    low = (rest - middle.astype(F32)).astype(BF)
    parts = []
    for group in range(scales.shape[0]):
        for piece in (high, middle, low):
            parts.append(piece[group : group + 1].astype(F32))
    parts.append(jnp.zeros((SCALE_ROWS - len(parts), LANES), F32))
    packed = jnp.concatenate(parts, axis=0).astype(BF)
    mixer_ref[0, rows:cut] = packed
    mixer_ref[1, rows:cut] = packed

    rows, width = gate_ref.shape[1], gate_ref.shape[0]
    full = width // LANES
    for j in range(full):
        cols = slice(j * LANES, (j + 1) * LANES)
        ffn_ref[2 * j * rows : (2 * j + 1) * rows] = gate_ref[cols].T.astype(BF)
        ffn_ref[(2 * j + 1) * rows : (2 * j + 2) * rows] = value_ref[cols].T.astype(BF)
    mixed = jnp.concatenate([gate_ref[full * LANES :], value_ref[full * LANES :]], axis=0)
    ffn_ref[2 * full * rows : (2 * full + 1) * rows] = mixed.T.astype(BF)
    ffn_ref[(2 * full + 1) * rows :] = down_ref[...].astype(BF)


def unpack_kernel(pos_ref, stack_ref, weight_ref, table_ref, out_ref):
    fs, mine = pos_ref[1], pos_ref[2]
    size = weight_ref.shape[0]
    cut = LANES + SCALE_ROWS
    for block in range(size):
        at = lax.rem(block - fs + size, size)
        below = at > size // 2
        places = jnp.where(below, size - at, at)
        k = lax.div(places + 1, 2)
        side = jnp.where(below, 3, 1) - lax.rem(places, 2)
        rows = block * LANES
        for half in range(2):
            piece = stack_ref.at[jnp.where(mine == half, 0, 1), k, side]
            weight_ref[block, :, half * LANES : (half + 1) * LANES] = piece[:LANES]
            out_ref[rows : rows + LANES // 2] = piece[cut:]
            rows += LANES // 2
            if half == 0:
                table_ref[block * SCALE_ROWS : (block + 1) * SCALE_ROWS] = piece[LANES:cut]


def mixer_kernel(pos_ref, *refs):
    tokens = refs[:8]
    (w_ref, table_ref, gain_ref, taps_ref, gates_ref, rate_ref, out_ref, x_ref, full_ref,
     scale_ref) = refs[8:]
    tp = pos_ref[0]
    width = tokens[0].shape[1]
    per_slot = width // LANES

    @pl.when(pl.program_id(0) == 0)
    def _():
        for slot, place in enumerate(SLOTS):
            device = slot_device(tp, place)
            for part in range(per_slot):
                base = slot * width + part * LANES
                full_ref[base : base + LANES] = w_ref[device * per_slot + part]
        table = table_ref[...]
        scale_ref[:, :LANES] = spread_scale(table, 0, 0)
        scale_ref[:, LANES:] = spread_scale(table, 0, 8)

    squares = None
    for slot in range(len(SLOTS)):
        values = tokens[slot][...].astype(F32)
        square = jnp.sum(values * values, axis=-1, keepdims=True)
        squares = square if squares is None else squares + square
    inverse = lax.rsqrt(squares * (1.0 / x_ref.shape[1]) + EPS)
    for slot, place in enumerate(SLOTS):
        values = tokens[slot][...].astype(F32)
        gain = gain_ref[slot_device(tp, place)]
        x_ref[:, slot * width : (slot + 1) * width] = (values * inverse * gain).astype(BF)
    both = jnp.dot(x_ref[...], full_ref[...], preferred_element_type=F32)
    taps = taps_ref[...] * scale_ref[:, :LANES]
    convolved = causal_mix(both[:, :LANES], taps).astype(BF)
    rates = jax.nn.sigmoid(jnp.dot(convolved, gates_ref[...], preferred_element_type=F32))
    log_decay = rates[:, :LANES] * rate_ref[...]
    driven = jnp.sqrt(minus_expm1(2.0 * log_decay)) * rates[:, LANES:] * convolved.astype(F32)
    states = scan_rows(jnp.exp(log_decay), driven)
    gelu_in = both[:, LANES:] * scale_ref[:, LANES:]
    out_ref[...] = (states * jax.nn.gelu(gelu_in)).astype(BF)


def cut_kernel(right_first, right_second, left_first, left_second, to_left_ref, to_right_ref):
    rows = right_first.shape[0]
    to_left_ref[:rows] = right_first[...]
    to_left_ref[rows:] = right_second[...]
    to_right_ref[:rows] = left_first[...]
    to_right_ref[rows:] = left_second[...]


def stack_kernel(
    own_first, own_second, right_first, right_second, far_top, far_bottom, left_first, left_second,
    stack_ref,
):
    rows = own_first.shape[0]
    pairs = ((0, own_first, own_second), (1, right_first, right_second), (3, left_first, left_second))
    for k, first, second in pairs:
        stack_ref[k, :rows] = first[...]
        stack_ref[k, rows:] = second[...]
    half = rows // 2
    middle = rows + own_second.shape[0] // 2
    stack_ref[2, :half] = far_top[:half]
    stack_ref[2, half:rows] = far_bottom[:half]
    stack_ref[2, rows:middle] = far_top[half:]
    stack_ref[2, middle:] = far_bottom[half:]


def scales_kernel(pos_ref, table_ref, taps_ref, cols_ref, mixed_ref, down_ref):
    tp = pos_ref[0]
    table = table_ref[...]
    per_slot = down_ref.shape[1] // LANES
    for slot, place in enumerate(SLOTS):
        device = slot_device(tp, place)
        for part in range(per_slot):
            block = device * per_slot + part
            base = (slot * per_slot + part) * LANES
            cols_ref[:, base : base + LANES] = spread_scale(table, 1, block * 8)
            if slot == 0:
                down_ref[:, base : base + LANES] = spread_scale(table, 2, block * 8)
    gate_at, value_at = 16, 60
    pairs = (mixed_ref.shape[1] // LANES) // 2
    for j in range(pairs):
        cols = slice(2 * j * LANES, (2 * j + 1) * LANES)
        mixed_ref[:, cols] = taps_ref[:, cols] * spread_scale(table, 0, gate_at + 8 * j)
        cols = slice((2 * j + 1) * LANES, (2 * j + 2) * LANES)
        mixed_ref[:, cols] = taps_ref[:, cols] * spread_scale(table, 0, value_at + 8 * j)
    cols = slice(2 * pairs * LANES, (2 * pairs + 1) * LANES)
    mixed_ref[:, cols] = taps_ref[:, cols] * spread_scale(
        table, 0, gate_at + 8 * pairs, value_at + 8 * pairs
    )


def out_kernel(pos_ref, *refs):
    tokens, gated, weights = refs[:8], refs[8:10], refs[10:12]
    scale_ref, gain_ref, normed_ref, own_ref, hidden_ref = refs[12:]
    tp = pos_ref[0]
    width = tokens[0].shape[1]
    per_slot = width // LANES

    def weight_columns(place):
        columns = []
        for part in range(per_slot):
            at = slot_device(tp, place) * per_slot + part
            rows = pl.ds(pl.multiple_of(at * LANES, LANES), LANES)
            blocks = [ref[k, rows] for ref in weights for k in range(HALF_SLOTS)]
            columns.append(jnp.concatenate(blocks, axis=0))
        return jnp.concatenate(columns, axis=1)

    states = jnp.concatenate([ref[k] for ref in gated for k in range(HALF_SLOTS)], axis=1)
    squares = None
    for slot, place in enumerate(SLOTS):
        cols = slice(slot * width, (slot + 1) * width)
        mixed = jnp.dot(states, weight_columns(place), preferred_element_type=F32)
        mixed = mixed * scale_ref[:, cols]
        hidden = (tokens[slot][...].astype(F32) + mixed).astype(BF)
        hidden_ref[:, cols] = hidden
        if slot == 0:
            own_ref[...] = hidden
        values = hidden.astype(F32)
        square = jnp.sum(values * values, axis=-1, keepdims=True)
        squares = square if squares is None else squares + square
    inverse = lax.rsqrt(squares * (1.0 / hidden_ref.shape[1]) + EPS)
    for slot, place in enumerate(SLOTS):
        device = slot_device(tp, place)
        values = hidden_ref[:, slot * width : (slot + 1) * width].astype(F32)
        normed_ref[device] = (values * inverse * gain_ref[device]).astype(BF)


def ffn_kernel(pos_ref, x_ref, taps_ref, w_ref, send_ref, keep_ref, hidden_ref):
    tp = pos_ref[0]
    count, _, width = x_ref.shape
    per_slot = width // LANES
    up_rows = taps_ref.shape[1]
    pairs = (up_rows // LANES) // 2
    depth = count * width

    def columns(j):
        return w_ref[:, j * LANES : (j + 1) * LANES].reshape(depth, LANES)

    x = jnp.concatenate([x_ref[k] for k in range(count)], axis=1)
    for j in range(pairs):
        weight = jnp.concatenate([columns(2 * j), columns(2 * j + 1)], axis=1)
        both = jnp.dot(x, weight, preferred_element_type=F32)
        both = causal_mix(both, taps_ref[:, 2 * j * LANES : (2 * j + 2) * LANES])
        gate = both[:, :LANES]
        hidden_ref[:, j * LANES : (j + 1) * LANES] = (
            gate * jax.nn.sigmoid(gate) * both[:, LANES:]
        ).astype(BF)
    both = jnp.dot(x, columns(2 * pairs), preferred_element_type=F32)
    both = causal_mix(both, taps_ref[:, 2 * pairs * LANES :])
    product = both * jax.nn.sigmoid(both) * pltpu.roll(both, LANES // 2, 1)
    hidden_ref[:, pairs * LANES :] = product[:, : LANES // 2].astype(BF)
    hidden = hidden_ref[...]
    for slot, place in enumerate(SLOTS):
        device = slot_device(tp, place)
        weight = jnp.concatenate(
            [w_ref[device * per_slot + part, up_rows:] for part in range(per_slot)], axis=1
        )
        term = jnp.dot(hidden, weight, preferred_element_type=F32).astype(BF)
        target = keep_ref if slot < HALF_SLOTS else send_ref
        target[slot % HALF_SLOTS] = term


def whole(array):
    rank = array.ndim
    return pl.BlockSpec(array.shape, lambda i, pos: (0,) * rank, pipeline_mode=pl.Buffered(1))


def row_block(rows, width):
    return pl.BlockSpec((rows, width), lambda i, pos: (i, 0))


def slab(count, rows, width, skip=0):
    return pl.BlockSpec((count, rows, width), lambda i, pos: (0, skip + i, 0))


def first_rows(count, rows, width):
    return pl.BlockSpec(
        (count, rows, width), lambda i, pos: (0, 0, 0), pipeline_mode=pl.Buffered(1)
    )


def call(kernel, position, steps, operands, in_specs, outs, out_specs, scratch, flops):
    size = sum(a.size * a.dtype.itemsize for a in operands)
    return pl.pallas_call(
        kernel,
        grid_spec=pltpu.PrefetchScalarGridSpec(
            num_scalar_prefetch=1,
            grid=(steps,),
            in_specs=in_specs,
            out_specs=out_specs,
            scratch_shapes=scratch,
        ),
        out_shape=outs,
        compiler_params=pltpu.CompilerParams(dimension_semantics=("arbitrary",)),
        cost_estimate=pl.CostEstimate(flops=flops, transcendentals=0, bytes_accessed=size),
    )(position, *operands)


def add_rounded(one, other):
    return (one.astype(F32) + other.astype(F32)).astype(BF)


def complete_tp(first, second, rights, lefts):
    halves = (first.shape[0] // 2, second.shape[0] // 2)
    part = jax.ShapeDtypeStruct((sum(halves), first.shape[1]), first.dtype)

    def half(rows, which):
        return pl.BlockSpec((rows, first.shape[1]), lambda i: (which, 0))

    to_left, to_right = pl.pallas_call(
        cut_kernel,
        grid=(1,),
        in_specs=[half(rows, which) for which in range(2) for rows in halves],
        out_specs=(half(sum(halves), 0), half(sum(halves), 0)),
        out_shape=(part, part),
        name="cut_far",
    )(*rights, *lefts)
    fars = (from_chip(to_left, 1), from_chip(to_right, -1))
    same = pl.pallas_call(
        stack_kernel,
        out_shape=jax.ShapeDtypeStruct((HALF_SLOTS, 2 * sum(halves), first.shape[1]), first.dtype),
        name="stack_chips",
    )(first, second, *rights, *fars, *lefts)
    return same, from_partner(same)


def block_diagonal(blocks):
    count, size, _ = blocks.shape
    rows = []
    for i in range(count):
        rows.append(jnp.pad(blocks[i], ((0, 0), (i * size, (count - 1 - i) * size))))
    return jnp.concatenate(rows, axis=0)


def per_device(
    tokens,
    mixer_gain,
    branch_weight,
    gelu_weight,
    branch_scale,
    gelu_scale,
    branch_taps,
    recur_gate,
    input_gate,
    decay_param,
    out_weight,
    out_scale,
    ffn_gain,
    upgate_weight,
    upval_weight,
    upgate_scale,
    upval_scale,
    upgate_taps,
    upval_taps,
    down_weight,
    down_scale,
):
    fs_size, tp_size = lax.axis_size("fs"), lax.axis_size("tp")
    rows, width = tokens.shape
    depth = width * tp_size
    steps = rows // SEQ_LEN
    mine = lax.rem(lax.axis_index("grp"), 2)
    position = jnp.stack([lax.axis_index("tp"), lax.axis_index("fs"), mine]).astype(jnp.int32)

    hidden_width = upgate_weight.shape[1]
    up_rows = 2 * hidden_width * upgate_weight.shape[0] // LANES
    ffn_rows = up_rows + hidden_width
    half_rows = LANES + SCALE_ROWS + LANES // 2
    packed_mixer, packed_ffn = pl.pallas_call(
        pack_kernel,
        out_shape=(
            jax.ShapeDtypeStruct((2, half_rows, LANES), BF),
            jax.ShapeDtypeStruct((ffn_rows, LANES), BF),
        ),
        name="pack",
    )(
        branch_weight,
        gelu_weight,
        out_weight,
        branch_scale,
        gelu_scale,
        upgate_scale,
        upval_scale,
        out_scale,
        down_scale,
        upgate_weight.T,
        upval_weight.T,
        down_weight,
    )
    ffn_weights = lax.all_gather(packed_ffn, "fs", axis=0, tiled=True)
    ffn_weights = ffn_weights.reshape(fs_size, ffn_rows, LANES)

    tokens, packed_mixer = lax.optimization_barrier((tokens, packed_mixer))
    token_slots = gather_directly(tokens)
    smem = pl.BlockSpec(memory_space=pltpu.SMEM)
    vmem = pl.BlockSpec(memory_space=pltpu.VMEM)
    mixer_weights, table, out_rows = pl.pallas_call(
        unpack_kernel,
        in_specs=[smem, vmem],
        out_specs=(vmem, vmem, vmem),
        out_shape=(
            jax.ShapeDtypeStruct((fs_size, LANES, 2 * LANES), BF),
            jax.ShapeDtypeStruct((fs_size * SCALE_ROWS, LANES), BF),
            jax.ShapeDtypeStruct((fs_size * LANES, LANES), BF),
        ),
        name="unpack",
    )(position, ring_fs(packed_mixer))
    out_right, out_left = near_chips(out_rows)

    gates = jnp.concatenate([block_diagonal(recur_gate), block_diagonal(input_gate)], axis=1)
    rate = (-8.0 * jax.nn.softplus(-decay_param))[None]
    mixer_gains = mixer_gain.reshape(tp_size, 1, width)
    ffn_gains = ffn_gain.reshape(tp_size, 1, width)
    token_specs = [row_block(SEQ_LEN, width)] * len(SLOTS)

    tail = (mixer_weights, table, mixer_gains, branch_taps, gates, rate)
    gated = call(
        mixer_kernel,
        position,
        steps,
        (*token_slots, *tail),
        token_specs + [whole(a) for a in tail],
        jax.ShapeDtypeStruct((rows, LANES), BF),
        row_block(SEQ_LEN, LANES),
        [
            pltpu.VMEM((SEQ_LEN, depth), BF),
            pltpu.VMEM((depth, 2 * LANES), BF),
            pltpu.VMEM((1, 2 * LANES), F32),
        ],
        2 * rows * depth * 2 * LANES,
    )
    near = lax.optimization_barrier((out_right, out_left, *near_chips(gated)))
    slots = complete_tp(out_rows, gated, near[0::2], near[1::2])

    edge = hidden_width // LANES * LANES
    tap_parts = []
    for j in range(hidden_width // LANES):
        tap_parts += [upgate_taps[:, j * LANES : (j + 1) * LANES]]
        tap_parts += [upval_taps[:, j * LANES : (j + 1) * LANES]]
    tap_parts += [upgate_taps[:, edge:], upval_taps[:, edge:]]
    ffn_taps = jnp.concatenate(tap_parts, axis=1)
    out_cols, scaled_taps, down_cols = pl.pallas_call(
        scales_kernel,
        in_specs=[smem, vmem, vmem],
        out_specs=(vmem, vmem, vmem),
        out_shape=(
            jax.ShapeDtypeStruct((1, depth), F32),
            jax.ShapeDtypeStruct(ffn_taps.shape, F32),
            jax.ShapeDtypeStruct((1, width), F32),
        ),
        name="spread_scales",
    )(position, table, ffn_taps)

    block = SEQ_LEN // 2
    tail = (out_cols, ffn_gains)
    normed, own_hidden = call(
        out_kernel,
        position,
        rows // block,
        (*token_slots, *slots, *slots, *tail),
        [row_block(block, width)] * len(SLOTS)
        + [slab(HALF_SLOTS, block, LANES, out_rows.shape[0] // block)] * CORES
        + [first_rows(HALF_SLOTS, out_rows.shape[0], LANES)] * CORES
        + [whole(a) for a in tail],
        (
            jax.ShapeDtypeStruct((tp_size, rows, width), BF),
            jax.ShapeDtypeStruct((rows, width), BF),
        ),
        (slab(tp_size, block, width), row_block(block, width)),
        [pltpu.VMEM((block, depth), BF)],
        2 * rows * tp_size * LANES * depth,
    )

    term = jax.ShapeDtypeStruct((HALF_SLOTS, rows, width), BF)
    send, keep = call(
        ffn_kernel,
        position,
        steps,
        (normed, scaled_taps, ffn_weights),
        [slab(tp_size, SEQ_LEN, width), whole(scaled_taps), whole(ffn_weights)],
        (term, term),
        (slab(HALF_SLOTS, SEQ_LEN, width), slab(HALF_SLOTS, SEQ_LEN, width)),
        [pltpu.VMEM((SEQ_LEN, hidden_width), BF)],
        6 * rows * depth * hidden_width,
    )
    received = from_partner(send)

    def added(slot, low, high):
        both = keep[slot, low:high].astype(F32) + received[slot, low:high].astype(F32)
        return both.astype(BF)

    half = rows // 2
    via_right = from_chip(added(2, 0, half), -1)
    via_left = from_chip(added(2, half, rows), 1)
    left_bottom = from_chip(added(1, half, rows), -1)
    right_top = from_chip(added(3, 0, half), 1)
    left_top = from_chip(add_rounded(added(1, 0, half), via_right), -1)
    right_bottom = from_chip(add_rounded(added(3, half, rows), via_left), 1)
    left_sum = jnp.concatenate([left_top, left_bottom], axis=0).astype(F32)
    right_sum = jnp.concatenate([right_top, right_bottom], axis=0).astype(F32)
    total = added(0, 0, rows).astype(F32) + left_sum + right_sum
    return (own_hidden.astype(F32) + total * down_cols).astype(BF)


def solution(mesh):
    in_specs = (
        P(("grp", "fs"), "tp"),
        P(),
        P("fs", "tp"),
        P("fs", "tp"),
        P("fs", "tp"),
        P("fs", "tp"),
        P(None, "tp"),
        P("tp", None, None),
        P("tp", None, None),
        P("tp"),
        P("tp", "fs"),
        P("fs", None),
        P(),
        P("fs", "tp"),
        P("fs", "tp"),
        P("fs", "tp"),
        P("fs", "tp"),
        P(None, "tp"),
        P(None, "tp"),
        P("tp", "fs"),
        P("fs", None),
    )
    out_specs = P(("grp", "fs"), "tp")

    return jax.shard_map(
        per_device, mesh=mesh, in_specs=in_specs, out_specs=out_specs, check_vma=False
    )
```

```python
import jax
import jax.numpy as jnp
from jax import lax
from jax.experimental import pallas as pl
from jax.experimental.pallas import tpu as pltpu
from jax.sharding import PartitionSpec as P


SEQ_LEN = 512
EPS = 1e-06
BF = jnp.bfloat16
F32 = jnp.float32
LANES = 128
CORES = 2
SLOTS = ((0, 0), (1, 0), (2, 0), (3, 0), (0, 1), (1, 1), (2, 1), (3, 1))
HALF_SLOTS = 4
SCALE_ROWS = 16
PIECES = 3


def from_chip(value, step):
    size = lax.axis_size("tp")
    chips = size // CORES
    pairs = [(i, ((i // CORES - step) % chips) * CORES + i % CORES) for i in range(size)]
    return lax.ppermute(value, "tp", pairs)


def from_partner(value):
    size = lax.axis_size("tp")
    return lax.ppermute(value, "tp", [(i, i ^ 1) for i in range(size)])


def near_chips(value):
    return from_chip(value, 1), from_chip(value, -1)


def far_chip(right, left):
    half = right.shape[0] // 2
    return from_chip(right[:half], 1), from_chip(left[half:], -1)


def complete_tp(value, right, left, far):
    same = jnp.stack([value, right, jnp.concatenate(far, axis=0), left])
    return same, from_partner(same)


def ring_fs(halves, beside_it):
    size, groups = lax.axis_size("fs"), lax.axis_size("grp")
    rounds = size // 4
    beside = [(i, i ^ 1) for i in range(groups)]
    mine = lax.rem(lax.axis_index("grp"), 2)
    own = lax.dynamic_index_in_dim(halves, mine, 0, keepdims=False)
    other = lax.dynamic_index_in_dim(halves, 1 - mine, 0, keepdims=False)
    stack = jnp.zeros((2, rounds + 1, 4, *own.shape), own.dtype)
    stack = lax.dynamic_update_slice(stack, own[None, None, None], (0, 0, 1, 0, 0))
    stack = lax.dynamic_update_slice(stack, other[None, None, None], (1, 0, 1, 0, 0))

    def from_place(value, step):
        return lax.ppermute(value, "fs", [(i, (i - step) % size) for i in range(size)])

    def further(above, below):
        return (
            from_place(above, 1),
            from_place(above, 2),
            from_place(below, -1),
            from_place(below, -2),
        )

    def held(stack, k, arrived):
        pieces = jnp.stack(arrived)
        stack = lax.dynamic_update_slice(stack, pieces[None, None], (0, k, 0, 0, 0))
        pieces = lax.ppermute(pieces, "grp", beside)
        return lax.dynamic_update_slice(stack, pieces[None, None], (1, k, 0, 0, 0))

    def step(k, state):
        stack, arrived = state
        following = further(arrived[1], arrived[3])
        return held(stack, k, arrived), following

    first = further(own, own)
    stack, arrived = lax.fori_loop(1, rounds, step, (stack, first))
    state = lax.optimization_barrier((stack, arrived, beside_it))
    stack, arrived, beside_it = state
    return held(stack, rounds, arrived), beside_it


def slot_device(tp, slot):
    step, other = slot
    core = lax.rem(tp, CORES)
    chip = lax.rem(lax.div(tp, CORES) + step + HALF_SLOTS, HALF_SLOTS)
    return chip * CORES + (1 - core if other else core)


def shift_rows(values, by, fill):
    rows = lax.broadcasted_iota(jnp.int32, values.shape, 0)
    return jnp.where(rows >= by, pltpu.roll(values, by, 0), fill)


def causal_mix(values, taps):
    count = taps.shape[0]
    total = values * taps[count - 1 : count]
    for by in range(1, count):
        total = total + shift_rows(values, by, 0.0) * taps[count - 1 - by : count - by]
    return total


def spread_scale(table, group, first, second=None):
    shape = (LANES, LANES)
    lane = lax.broadcasted_iota(jnp.int32, shape, 1)
    row = lax.broadcasted_iota(jnp.int32, shape, 0)
    wanted = first + lax.shift_right_logical(lane, 4)
    if second is not None:
        wanted = jnp.where(lane < LANES // 2, wanted, second + lax.shift_right_logical(lane, 4) - 4)
    pick = jnp.where(row == wanted, 1.0, 0.0).astype(BF)
    hits = jnp.dot(table, pick, preferred_element_type=F32)
    row = lax.broadcasted_iota(jnp.int32, hits.shape, 0)
    lane = lax.broadcasted_iota(jnp.int32, hits.shape, 1)
    owner = lax.shift_right_logical(row, 4)
    local = lax.bitwise_and(row, SCALE_ROWS - 1)
    keep = (
        (owner == lax.bitwise_and(lane, 15))
        & (local >= group * PIECES)
        & (local < group * PIECES + PIECES)
    )
    return jnp.sum(jnp.where(keep, hits, 0.0), axis=0, keepdims=True)


def minus_expm1(x):
    series = x * (
        1.0
        + x
        * (0.5 + x * (1.0 / 6 + x * (1.0 / 24 + x * (1.0 / 120 + x * (1.0 / 720 + x / 5040)))))
    )
    return jnp.where(x > -0.5, -series, 1.0 - jnp.exp(x))


def scan_rows(factors, inputs):
    by = 1
    while by < factors.shape[0]:
        if by < 8:
            before_f, before_i = shift_rows(factors, by, 1.0), shift_rows(inputs, by, 0.0)
        else:
            top = (by, factors.shape[1])
            before_f = jnp.concatenate([jnp.ones(top, F32), factors[:-by]], axis=0)
            before_i = jnp.concatenate([jnp.zeros(top, F32), inputs[:-by]], axis=0)
        inputs = factors * before_i + inputs
        factors = factors * before_f
        by *= 2
    return inputs


def pack_kernel(branch_ref, gelu_ref, out_ref, *refs):
    narrow, wide = refs[:4], refs[4:6]
    gate_ref, value_ref, down_ref, mixer_ref, ffn_ref = refs[6:]
    rows = branch_ref.shape[0]
    cut = rows + SCALE_ROWS
    mixer_ref[0, 0:rows] = branch_ref[...].astype(BF)
    mixer_ref[1, 0:rows] = gelu_ref[...].astype(BF)
    mixer_ref[0, cut:] = out_ref[: rows // 2].astype(BF)
    mixer_ref[1, cut:] = out_ref[rows // 2 :].astype(BF)
    small = [ref[...] for ref in narrow]
    small.append(jnp.zeros((1, LANES - sum(v.shape[1] for v in small)), F32))
    scales = jnp.concatenate([jnp.concatenate(small, axis=1), *[ref[...] for ref in wide]], axis=0)
    high = scales.astype(BF)
    rest = scales - high.astype(F32)
    middle = rest.astype(BF)
    low = (rest - middle.astype(F32)).astype(BF)
    parts = []
    for group in range(scales.shape[0]):
        for piece in (high, middle, low):
            parts.append(piece[group : group + 1].astype(F32))
    parts.append(jnp.zeros((SCALE_ROWS - len(parts), LANES), F32))
    packed = jnp.concatenate(parts, axis=0).astype(BF)
    mixer_ref[0, rows:cut] = packed
    mixer_ref[1, rows:cut] = packed

    rows, width = gate_ref.shape[1], gate_ref.shape[0]
    full = width // LANES
    for j in range(full):
        cols = slice(j * LANES, (j + 1) * LANES)
        ffn_ref[2 * j * rows : (2 * j + 1) * rows] = gate_ref[cols].T.astype(BF)
        ffn_ref[(2 * j + 1) * rows : (2 * j + 2) * rows] = value_ref[cols].T.astype(BF)
    mixed = jnp.concatenate([gate_ref[full * LANES :], value_ref[full * LANES :]], axis=0)
    ffn_ref[2 * full * rows : (2 * full + 1) * rows] = mixed.T.astype(BF)
    ffn_ref[(2 * full + 1) * rows :] = down_ref[...].astype(BF)


def unpack_kernel(pos_ref, stack_ref, weight_ref, table_ref, out_ref):
    fs, mine = pos_ref[1], pos_ref[2]
    size = weight_ref.shape[0]
    cut = LANES + SCALE_ROWS
    for block in range(size):
        at = lax.rem(block - fs + size, size)
        below = at > size // 2
        places = jnp.where(below, size - at, at)
        k = lax.div(places + 1, 2)
        side = jnp.where(below, 3, 1) - lax.rem(places, 2)
        rows = block * LANES
        for half in range(2):
            piece = stack_ref.at[jnp.where(mine == half, 0, 1), k, side]
            weight_ref[block, :, half * LANES : (half + 1) * LANES] = piece[:LANES]
            out_ref[rows : rows + LANES // 2] = piece[cut:]
            rows += LANES // 2
            if half == 0:
                table_ref[block * SCALE_ROWS : (block + 1) * SCALE_ROWS] = piece[LANES:cut]


def mixer_kernel(pos_ref, *refs):
    tokens = [ref.at[k] for ref in refs[:2] for k in range(HALF_SLOTS)]
    (w_ref, table_ref, gain_ref, taps_ref, gates_ref, rate_ref, out_ref, x_ref, full_ref,
     scale_ref) = refs[2:]
    tp = pos_ref[0]
    width = refs[0].shape[2]
    per_slot = width // LANES

    @pl.when(pl.program_id(0) == 0)
    def _():
        for slot, place in enumerate(SLOTS):
            device = slot_device(tp, place)
            for part in range(per_slot):
                base = slot * width + part * LANES
                full_ref[base : base + LANES] = w_ref[device * per_slot + part]
        table = table_ref[...]
        scale_ref[:, :LANES] = spread_scale(table, 0, 0)
        scale_ref[:, LANES:] = spread_scale(table, 0, 8)

    squares = None
    for slot in range(len(SLOTS)):
        values = tokens[slot][...].astype(F32)
        square = jnp.sum(values * values, axis=-1, keepdims=True)
        squares = square if squares is None else squares + square
    inverse = lax.rsqrt(squares * (1.0 / x_ref.shape[1]) + EPS)
    for slot, place in enumerate(SLOTS):
        values = tokens[slot][...].astype(F32)
        gain = gain_ref[slot_device(tp, place)]
        x_ref[:, slot * width : (slot + 1) * width] = (values * inverse * gain).astype(BF)
    both = jnp.dot(x_ref[...], full_ref[...], preferred_element_type=F32)
    taps = taps_ref[...] * scale_ref[:, :LANES]
    convolved = causal_mix(both[:, :LANES], taps).astype(BF)
    rates = jax.nn.sigmoid(jnp.dot(convolved, gates_ref[...], preferred_element_type=F32))
    log_decay = rates[:, :LANES] * rate_ref[...]
    driven = jnp.sqrt(minus_expm1(2.0 * log_decay)) * rates[:, LANES:] * convolved.astype(F32)
    states = scan_rows(jnp.exp(log_decay), driven)
    gelu_in = both[:, LANES:] * scale_ref[:, LANES:]
    out_ref[...] = (states * jax.nn.gelu(gelu_in)).astype(BF)


def scales_kernel(pos_ref, table_ref, taps_ref, cols_ref, mixed_ref, down_ref):
    tp = pos_ref[0]
    table = table_ref[...]
    per_slot = down_ref.shape[1] // LANES
    for slot, place in enumerate(SLOTS):
        device = slot_device(tp, place)
        for part in range(per_slot):
            block = device * per_slot + part
            base = (slot * per_slot + part) * LANES
            cols_ref[:, base : base + LANES] = spread_scale(table, 1, block * 8)
            if slot == 0:
                down_ref[:, base : base + LANES] = spread_scale(table, 2, block * 8)
    gate_at, value_at = 16, 60
    pairs = (mixed_ref.shape[1] // LANES) // 2
    for j in range(pairs):
        cols = slice(2 * j * LANES, (2 * j + 1) * LANES)
        mixed_ref[:, cols] = taps_ref[:, cols] * spread_scale(table, 0, gate_at + 8 * j)
        cols = slice((2 * j + 1) * LANES, (2 * j + 2) * LANES)
        mixed_ref[:, cols] = taps_ref[:, cols] * spread_scale(table, 0, value_at + 8 * j)
    cols = slice(2 * pairs * LANES, (2 * pairs + 1) * LANES)
    mixed_ref[:, cols] = taps_ref[:, cols] * spread_scale(
        table, 0, gate_at + 8 * pairs, value_at + 8 * pairs
    )


def out_kernel(pos_ref, *refs):
    tokens = [ref.at[k] for ref in refs[:2] for k in range(HALF_SLOTS)]
    gated, weights = refs[2:4], refs[4:6]
    scale_ref, gain_ref, normed_ref, own_ref, hidden_ref = refs[6:]
    tp = pos_ref[0]
    width = refs[0].shape[2]
    per_slot = width // LANES

    def weight_columns(place):
        columns = []
        for part in range(per_slot):
            at = slot_device(tp, place) * per_slot + part
            rows = pl.ds(pl.multiple_of(at * LANES, LANES), LANES)
            blocks = [ref[k, rows] for ref in weights for k in range(HALF_SLOTS)]
            columns.append(jnp.concatenate(blocks, axis=0))
        return jnp.concatenate(columns, axis=1)

    states = jnp.concatenate([ref[k] for ref in gated for k in range(HALF_SLOTS)], axis=1)
    squares = None
    for slot, place in enumerate(SLOTS):
        cols = slice(slot * width, (slot + 1) * width)
        mixed = jnp.dot(states, weight_columns(place), preferred_element_type=F32)
        mixed = mixed * scale_ref[:, cols]
        hidden = (tokens[slot][...].astype(F32) + mixed).astype(BF)
        hidden_ref[:, cols] = hidden
        if slot == 0:
            own_ref[...] = hidden
        values = hidden.astype(F32)
        square = jnp.sum(values * values, axis=-1, keepdims=True)
        squares = square if squares is None else squares + square
    inverse = lax.rsqrt(squares * (1.0 / hidden_ref.shape[1]) + EPS)
    for slot, place in enumerate(SLOTS):
        device = slot_device(tp, place)
        values = hidden_ref[:, slot * width : (slot + 1) * width].astype(F32)
        normed_ref[device] = (values * inverse * gain_ref[device]).astype(BF)


def ffn_kernel(pos_ref, x_ref, taps_ref, w_ref, send_ref, keep_ref, hidden_ref):
    tp = pos_ref[0]
    count, _, width = x_ref.shape
    per_slot = width // LANES
    up_rows = taps_ref.shape[1]
    pairs = (up_rows // LANES) // 2
    depth = count * width

    def columns(j):
        return w_ref[:, j * LANES : (j + 1) * LANES].reshape(depth, LANES)

    x = jnp.concatenate([x_ref[k] for k in range(count)], axis=1)
    for j in range(pairs):
        weight = jnp.concatenate([columns(2 * j), columns(2 * j + 1)], axis=1)
        both = jnp.dot(x, weight, preferred_element_type=F32)
        both = causal_mix(both, taps_ref[:, 2 * j * LANES : (2 * j + 2) * LANES])
        gate = both[:, :LANES]
        hidden_ref[:, j * LANES : (j + 1) * LANES] = (
            gate * jax.nn.sigmoid(gate) * both[:, LANES:]
        ).astype(BF)
    both = jnp.dot(x, columns(2 * pairs), preferred_element_type=F32)
    both = causal_mix(both, taps_ref[:, 2 * pairs * LANES :])
    product = both * jax.nn.sigmoid(both) * pltpu.roll(both, LANES // 2, 1)
    hidden_ref[:, pairs * LANES :] = product[:, : LANES // 2].astype(BF)
    hidden = hidden_ref[...]
    for slot, place in enumerate(SLOTS):
        device = slot_device(tp, place)
        weight = jnp.concatenate(
            [w_ref[device * per_slot + part, up_rows:] for part in range(per_slot)], axis=1
        )
        term = jnp.dot(hidden, weight, preferred_element_type=F32).astype(BF)
        target = keep_ref if slot < HALF_SLOTS else send_ref
        target[slot % HALF_SLOTS] = term


def whole(array):
    rank = array.ndim
    return pl.BlockSpec(array.shape, lambda i, pos: (0,) * rank, pipeline_mode=pl.Buffered(1))


def row_block(rows, width):
    return pl.BlockSpec((rows, width), lambda i, pos: (i, 0))


def slab(count, rows, width):
    return pl.BlockSpec((count, rows, width), lambda i, pos: (0, i, 0))


def call(kernel, position, steps, operands, in_specs, outs, out_specs, scratch, flops):
    size = sum(a.size * a.dtype.itemsize for a in operands)
    return pl.pallas_call(
        kernel,
        grid_spec=pltpu.PrefetchScalarGridSpec(
            num_scalar_prefetch=1,
            grid=(steps,),
            in_specs=in_specs,
            out_specs=out_specs,
            scratch_shapes=scratch,
        ),
        out_shape=outs,
        compiler_params=pltpu.CompilerParams(dimension_semantics=("arbitrary",)),
        cost_estimate=pl.CostEstimate(flops=flops, transcendentals=0, bytes_accessed=size),
    )(position, *operands)


def add_rounded(one, other):
    return (one.astype(F32) + other.astype(F32)).astype(BF)


def block_diagonal(blocks):
    count, size, _ = blocks.shape
    rows = []
    for i in range(count):
        rows.append(jnp.pad(blocks[i], ((0, 0), (i * size, (count - 1 - i) * size))))
    return jnp.concatenate(rows, axis=0)


def per_device(
    tokens,
    mixer_gain,
    branch_weight,
    gelu_weight,
    branch_scale,
    gelu_scale,
    branch_taps,
    recur_gate,
    input_gate,
    decay_param,
    out_weight,
    out_scale,
    ffn_gain,
    upgate_weight,
    upval_weight,
    upgate_scale,
    upval_scale,
    upgate_taps,
    upval_taps,
    down_weight,
    down_scale,
):
    fs_size, tp_size = lax.axis_size("fs"), lax.axis_size("tp")
    rows, width = tokens.shape
    depth = width * tp_size
    steps = rows // SEQ_LEN
    mine = lax.rem(lax.axis_index("grp"), 2)
    position = jnp.stack([lax.axis_index("tp"), lax.axis_index("fs"), mine]).astype(jnp.int32)

    hidden_width = upgate_weight.shape[1]
    up_rows = 2 * hidden_width * upgate_weight.shape[0] // LANES
    ffn_rows = up_rows + hidden_width
    half_rows = LANES + SCALE_ROWS + LANES // 2
    packed_mixer, packed_ffn = pl.pallas_call(
        pack_kernel,
        out_shape=(
            jax.ShapeDtypeStruct((2, half_rows, LANES), BF),
            jax.ShapeDtypeStruct((ffn_rows, LANES), BF),
        ),
        name="pack",
    )(
        branch_weight,
        gelu_weight,
        out_weight,
        branch_scale,
        gelu_scale,
        upgate_scale,
        upval_scale,
        out_scale,
        down_scale,
        upgate_weight.T,
        upval_weight.T,
        down_weight,
    )
    ffn_weights = lax.all_gather(packed_ffn, "fs", axis=0, tiled=True)
    ffn_weights = ffn_weights.reshape(fs_size, ffn_rows, LANES)

    tokens, packed_mixer = lax.optimization_barrier((tokens, packed_mixer))
    other_chips = [from_chip(tokens, step) for step in (1, 2, 3)]
    stacked, other_chips = ring_fs(packed_mixer, other_chips)
    same_core = jnp.stack([tokens, *other_chips])
    token_slots = (same_core, from_partner(same_core))
    smem = pl.BlockSpec(memory_space=pltpu.SMEM)
    vmem = pl.BlockSpec(memory_space=pltpu.VMEM)
    mixer_weights, table, out_rows = pl.pallas_call(
        unpack_kernel,
        in_specs=[smem, vmem],
        out_specs=(vmem, vmem, vmem),
        out_shape=(
            jax.ShapeDtypeStruct((fs_size, LANES, 2 * LANES), BF),
            jax.ShapeDtypeStruct((fs_size * SCALE_ROWS, LANES), BF),
            jax.ShapeDtypeStruct((fs_size * LANES, LANES), BF),
        ),
        name="unpack",
    )(position, stacked)
    out_right, out_left = near_chips(out_rows)

    gates = jnp.concatenate([block_diagonal(recur_gate), block_diagonal(input_gate)], axis=1)
    rate = (-8.0 * jax.nn.softplus(-decay_param))[None]
    mixer_gains = mixer_gain.reshape(tp_size, 1, width)
    ffn_gains = ffn_gain.reshape(tp_size, 1, width)
    token_specs = [slab(HALF_SLOTS, SEQ_LEN, width)] * CORES

    tail = (mixer_weights, table, mixer_gains, branch_taps, gates, rate)
    gated = call(
        mixer_kernel,
        position,
        steps,
        (*token_slots, *tail),
        token_specs + [whole(a) for a in tail],
        jax.ShapeDtypeStruct((rows, LANES), BF),
        row_block(SEQ_LEN, LANES),
        [
            pltpu.VMEM((SEQ_LEN, depth), BF),
            pltpu.VMEM((depth, 2 * LANES), BF),
            pltpu.VMEM((1, 2 * LANES), F32),
        ],
        2 * rows * depth * 2 * LANES,
    )
    near = lax.optimization_barrier((out_right, out_left, *near_chips(gated)))
    far = lax.optimization_barrier((*far_chip(*near[2:]), *far_chip(*near[:2])))
    gated_slots = complete_tp(gated, *near[2:], far[:2])
    out_slots = complete_tp(out_rows, *near[:2], far[2:])

    edge = hidden_width // LANES * LANES
    tap_parts = []
    for j in range(hidden_width // LANES):
        tap_parts += [upgate_taps[:, j * LANES : (j + 1) * LANES]]
        tap_parts += [upval_taps[:, j * LANES : (j + 1) * LANES]]
    tap_parts += [upgate_taps[:, edge:], upval_taps[:, edge:]]
    ffn_taps = jnp.concatenate(tap_parts, axis=1)
    out_cols, scaled_taps, down_cols = pl.pallas_call(
        scales_kernel,
        in_specs=[smem, vmem, vmem],
        out_specs=(vmem, vmem, vmem),
        out_shape=(
            jax.ShapeDtypeStruct((1, depth), F32),
            jax.ShapeDtypeStruct(ffn_taps.shape, F32),
            jax.ShapeDtypeStruct((1, width), F32),
        ),
        name="spread_scales",
    )(position, table, ffn_taps)

    block = SEQ_LEN // 2
    tail = (out_cols, ffn_gains)
    normed, own_hidden = call(
        out_kernel,
        position,
        rows // block,
        (*token_slots, *gated_slots, *out_slots, *tail),
        [slab(HALF_SLOTS, block, width)] * CORES
        + [slab(HALF_SLOTS, block, LANES)] * CORES
        + [whole(a) for a in (*out_slots, *tail)],
        (
            jax.ShapeDtypeStruct((tp_size, rows, width), BF),
            jax.ShapeDtypeStruct((rows, width), BF),
        ),
        (slab(tp_size, block, width), row_block(block, width)),
        [pltpu.VMEM((block, depth), BF)],
        2 * rows * tp_size * LANES * depth,
    )

    term = jax.ShapeDtypeStruct((HALF_SLOTS, rows, width), BF)
    send, keep = call(
        ffn_kernel,
        position,
        steps,
        (normed, scaled_taps, ffn_weights),
        [slab(tp_size, SEQ_LEN, width), whole(scaled_taps), whole(ffn_weights)],
        (term, term),
        (slab(HALF_SLOTS, SEQ_LEN, width), slab(HALF_SLOTS, SEQ_LEN, width)),
        [pltpu.VMEM((SEQ_LEN, hidden_width), BF)],
        6 * rows * depth * hidden_width,
    )
    received = from_partner(send)

    def added(slot, low, high):
        both = keep[slot, low:high].astype(F32) + received[slot, low:high].astype(F32)
        return both.astype(BF)

    half = rows // 2
    via_right = from_chip(added(2, 0, half), -1)
    via_left = from_chip(added(2, half, rows), 1)
    left_bottom = from_chip(added(1, half, rows), -1)
    right_top = from_chip(added(3, 0, half), 1)
    left_top = from_chip(add_rounded(added(1, 0, half), via_right), -1)
    right_bottom = from_chip(add_rounded(added(3, half, rows), via_left), 1)
    left_sum = jnp.concatenate([left_top, left_bottom], axis=0).astype(F32)
    right_sum = jnp.concatenate([right_top, right_bottom], axis=0).astype(F32)
    total = added(0, 0, rows).astype(F32) + left_sum + right_sum
    return (own_hidden.astype(F32) + total * down_cols).astype(BF)


def solution(mesh):
    in_specs = (
        P(("grp", "fs"), "tp"),
        P(),
        P("fs", "tp"),
        P("fs", "tp"),
        P("fs", "tp"),
        P("fs", "tp"),
        P(None, "tp"),
        P("tp", None, None),
        P("tp", None, None),
        P("tp"),
        P("tp", "fs"),
        P("fs", None),
        P(),
        P("fs", "tp"),
        P("fs", "tp"),
        P("fs", "tp"),
        P("fs", "tp"),
        P(None, "tp"),
        P(None, "tp"),
        P("tp", "fs"),
        P("fs", None),
    )
    out_specs = P(("grp", "fs"), "tp")

    return jax.shard_map(
        per_device, mesh=mesh, in_specs=in_specs, out_specs=out_specs, check_vma=False
    )
```
